512 devices in a mesh: grp: 2 (over y), sp: 16 (over z), tp: 16 (over x, core).
Axes of the slice: x: 8, y: 2, z: 16, core: 2. Of those that a mesh axis runs over, the one named last changes fastest.
The devices are a block of a 8x16x16 slice.
Arguments:
- hidden_in: bfloat16 [20480, 4096], P(('grp', 'sp'), 'tp'), parts along dimension 0, may hold values from -64 to 64
- norm_gain: float32 [2, 4096], replicated, may hold values from 0.1 to 1.9
- w_pool_in: bfloat16 [2, 4096, 1024], P(None, 'sp', 'tp'), may hold values from -0.09375 to 0.09375
- w_pool_gate: bfloat16 [2, 4096, 1024], P(None, 'sp', 'tp'), may hold values from -0.09375 to 0.09375
- group_mix: bfloat16 [2, 16, 64, 64], replicated, may hold values from -0.75 to 0.75
- w_out: bfloat16 [2, 1024, 4096], P(None, 'sp', 'tp'), may hold values from -0.1875 to 0.1875
Outputs:
- hidden_out: bfloat16 [20480, 4096], P(('grp', 'sp'), 'tp'), parts along dimension 0
The draws below stay inside these ranges and needn't reach their ends.
There are 2 independent parts, one for each index of `grp`. The reference program is written for one: setup_inputs(seed, part) draws one part's arguments, and reference() takes and returns one part's arrays. A program takes and returns all parts, laid end to end along the dimension named above; an argument that names none is the same for every part. Nothing has to cross between parts.
All inputs are finite; a program needn't handle non-finite values.
Results may differ from the reference program's by a relative error of at most 0.012.
Values may be sent and summed in bfloat16 or wider, within the bound.
No kernel may reach another device: no remote copies, remote signals or barrier semaphores. Data moves between devices by JAX's collectives and lax.ppermute only.
A program may use at most 64 MiB of HBM per device.

```python
import jax
import jax.numpy as jnp
from jax import lax

D = 4096
DP = 1024
GROUP = 64
GROUPS = 16
LAYERS = 2
TOKENS = 10240


def draw_hidden_in(key, part):
    base_key = jax.random.fold_in(key, 11)
    key_one, key_two = jax.random.split(base_key, 2)
    values = jax.random.normal(key_one, (TOKENS, D), jnp.float32)
    ramp = jnp.arange(D, dtype=jnp.float32) / D
    column_scale = jnp.exp(jnp.log(10.0) * (0.6 * ramp + 0.4 * jax.random.uniform(key_two, (D,), jnp.float32))) * 0.3162
    values = jnp.clip(values * column_scale[None, :], -60.0, 60.0)
    return values.astype(jnp.bfloat16)


def steps_of(key, extent, cuts, low, largest):
    loudness = 1.0
    for dim, parts in cuts:
        steps = jax.random.uniform(jax.random.fold_in(jax.random.fold_in(key, 6), dim), (parts,), jnp.float32, low / len(cuts), largest / len(cuts))
        loudness = loudness * jnp.repeat(jnp.exp(steps), extent[dim] // parts).reshape((-1,) + (1,) * (len(extent) - 1 - dim))
    return loudness


def scatter_about(rng, shape, scale, most, shards=(), kind=jnp.bfloat16):
    array = scale * jax.random.normal(rng, shape, jnp.float32)
    if shards:
        array = array * steps_of(rng, shape, shards, -0.22, 0.18)
    return jnp.clip(array, -most, most).astype(kind)


def setup_inputs(seed: int = 0, part: int = 0) -> dict:
    arg_keys = jax.random.split(jax.random.key(seed), 7)
    own_keys = jax.random.split(jax.random.fold_in(arg_keys[6], part), 7)
    hidden_in = draw_hidden_in(jax.random.fold_in(jax.random.fold_in(arg_keys[6], part), 71), part)
    norm_gain = jnp.clip(1.0 + 0.18 * jax.random.normal(arg_keys[1], (LAYERS, D), jnp.float32), 0.1, 1.9)
    w_pool_in = scatter_about(arg_keys[2], (LAYERS, D, DP), D ** -0.5, 0.09375, ((1, 16), (2, 16)))
    w_pool_gate = scatter_about(arg_keys[3], (LAYERS, D, DP), D ** -0.5, 0.09375, ((1, 16), (2, 16)))
    group_mix = scatter_about(arg_keys[4], (LAYERS, GROUPS, GROUP, GROUP), GROUP ** -0.5, 0.75)
    w_out = scatter_about(arg_keys[5], (LAYERS, DP, D), DP ** -0.5, 0.1875, ((1, 16), (2, 16)))
    return dict(hidden_in=hidden_in, norm_gain=norm_gain, w_pool_in=w_pool_in, w_pool_gate=w_pool_gate, group_mix=group_mix, w_out=w_out)


norm_eps = 1e-06

def reference(hidden_in, norm_gain, w_pool_in, w_pool_gate, group_mix, w_out):
    resid = hidden_in
    position = jnp.arange(TOKENS, dtype=jnp.int32)
    for layer in range(LAYERS):
        resid_f = resid.astype(jnp.float32)
        mean_sq = lax.optimization_barrier(jnp.mean(resid_f * resid_f, axis=1, keepdims=True))
        normed = (resid_f * lax.rsqrt(mean_sq + norm_eps) * norm_gain[layer]).astype(jnp.bfloat16)
        pool_in = jnp.dot(normed, w_pool_in[layer], preferred_element_type=jnp.float32).astype(jnp.bfloat16)
        gate = jnp.dot(normed, w_pool_gate[layer], preferred_element_type=jnp.float32).astype(jnp.bfloat16)
        grouped = pool_in.astype(jnp.float32).reshape(TOKENS, GROUPS, GROUP)
        running = jnp.concatenate([jnp.zeros((1, GROUPS, GROUP), jnp.float32), jnp.cumsum(grouped, axis=0)], axis=0)
        pieces = []
        for group_id in range(GROUPS):
            half = 2 ** (group_id % 4)
            lower = jnp.clip(position - half, 0, TOKENS).astype(jnp.int32)
            upper = jnp.clip(position + half, 0, TOKENS).astype(jnp.int32)
            window_sum = running[upper, group_id] - running[lower, group_id]
            counted = (upper - lower).astype(jnp.float32)[:, None]
            pieces.append(window_sum / counted - grouped[:, group_id])
        pooled = jnp.stack(pieces, axis=1).astype(jnp.bfloat16)
        mixed = jnp.einsum('tgc,gcd->tgd', pooled.astype(jnp.float32), group_mix[layer].astype(jnp.float32))
        mixed = mixed.reshape(TOKENS, DP)
        branch = (mixed * jax.nn.silu(gate.astype(jnp.float32))).astype(jnp.bfloat16)
        resid = (resid_f + jnp.dot(branch, w_out[layer], preferred_element_type=jnp.float32)).astype(jnp.bfloat16)
    return resid
```

```python
import jax
import jax.numpy as jnp
from jax import lax
from jax.sharding import PartitionSpec as P

GROUP = 64
CORES = 2
REACH = 8
norm_eps = 1e-06
bf16 = jnp.bfloat16
f32 = jnp.float32


def sent_to_all(array, axis):
    copies = jnp.broadcast_to(array, (lax.axis_size(axis), *array.shape))
    return lax.all_to_all(copies, axis, split_axis=0, concat_axis=0, tiled=True)


def swap_cores(array):
    size = lax.axis_size("tp")
    return lax.ppermute(array, "tp", [(i, i ^ 1) for i in range(size)])


def shifted_over_chips(array, step):
    size = lax.axis_size("tp")
    return lax.ppermute(array, "tp", [(i, (i + CORES * step) % size) for i in range(size)])


def same_core_blocks(block):
    chips = lax.axis_size("tp") // CORES
    chip = lax.axis_index("tp") // CORES
    out = jnp.zeros((chips, *block.shape), block.dtype)
    origin = (0,) * block.ndim
    out = lax.dynamic_update_slice(out, block[None], (chip, *origin))
    right = left = block
    for step in range(1, chips // 2 + 1):
        right = shifted_over_chips(right, 1)
        out = lax.dynamic_update_slice(out, right[None], ((chip - step) % chips, *origin))
        if step < chips - chips // 2:
            left = shifted_over_chips(left, -1)
            out = lax.dynamic_update_slice(out, left[None], ((chip + step) % chips, *origin))
    return out


def dot0(left, right):
    return lax.dot_general(left, right, (((0,), (0,)), ((), ())), preferred_element_type=f32)


def window(array, start, length):
    return lax.slice_in_dim(array, start, start + length, axis=1)


def mixed_branch(sums, scaling, mix, first_position, total_rows, code):
    rows = sums.shape[1] - 2 * REACH
    chans = sums.shape[0] // 2
    scaled = (sums * scaling[None, :]).astype(bf16).astype(f32)
    pool_in = scaled[:chans]
    gate = window(scaled[chans:], REACH, rows)
    position = first_position + jnp.arange(rows, dtype=jnp.int32)
    half = jnp.left_shift(1, code)
    counted = jnp.minimum(position + half, total_rows) - jnp.maximum(position - half, 0)
    counted = jnp.maximum(counted, 1).astype(f32)
    running = pool_in
    total = None
    for code_value, size in enumerate((1, 2, 4, 8)):
        width = running.shape[1] - size
        running = window(running, 0, width) + window(running, size, width)
        picked = window(running, REACH - size, rows)
        total = picked if total is None else jnp.where(code == code_value, picked, total)
    pooled = (total / counted[None, :] - window(pool_in, REACH, rows)).astype(bf16)
    mixed = dot0(mix, pooled)
    return (mixed * jax.nn.silu(gate)).astype(bf16)


def local(hidden_in, norm_gain, w_pool_in, w_pool_gate, group_mix, w_out):
    rows, cols = hidden_in.shape
    chans = w_pool_in.shape[2]
    depth = w_pool_in.shape[1]
    out_rows = w_out.shape[1]
    col_rank = lax.axis_index("tp")
    row_rank = lax.axis_index("sp")
    tp_size = lax.axis_size("tp")
    sp_size = lax.axis_size("sp")
    core = col_rank % CORES
    total_rows = rows * sp_size
    full_width = cols * tp_size
    code = col_rank % 4
    halo = 2 * REACH
    ext_rows = rows + 2 * halo

    packed = []
    for layer in range(2):
        gain = lax.dynamic_slice_in_dim(norm_gain[layer], row_rank * depth, depth)[:, None]
        both = jnp.concatenate([w_pool_in[layer], w_pool_gate[layer]], axis=1)
        packed.append((both.astype(f32) * gain).astype(bf16))
    lanes = 2 * chans
    for layer in range(2):
        packed += [w_out[layer][:, i : i + lanes] for i in range(0, cols, lanes)]
    gathered = lax.all_gather(jnp.concatenate(packed, axis=0), "sp", axis=0, tiled=False)
    w_first, w_second = (
        gathered[:, i * depth : (i + 1) * depth].reshape(sp_size // CORES, CORES, depth, lanes) for i in range(2)
    )
    outs = []
    at = 2 * depth
    for layer in range(2):
        pieces = []
        for i in range(0, cols, lanes):
            pieces.append(gathered[:, at : at + out_rows].reshape(sp_size * out_rows, lanes))
            at += out_rows
        outs.append(jnp.concatenate(pieces, axis=1))

    up = [(i, i + 1) for i in range(sp_size - 1)]
    down = [(j, i) for i, j in up]
    before = lax.ppermute(hidden_in[rows - halo :], "sp", up)
    after = lax.ppermute(hidden_in[:halo], "sp", down)
    block = jnp.concatenate([before, hidden_in, after, w_out[0]], axis=0).T
    mine = same_core_blocks(block)
    other = swap_cores(mine)
    even = jnp.where(core == 0, mine, other)
    odd = jnp.where(core == 0, other, mine)

    def squares(array):
        part = window(array.reshape(-1, array.shape[-1]), 0, ext_rows).astype(f32)
        return jnp.sum(part * part, axis=0)

    scaling = lax.rsqrt((squares(even) + squares(odd)) / full_width + norm_eps)

    def product(weight, length):
        total = 0
        for i, part in enumerate((even, odd)):
            part = window(part.reshape(-1, part.shape[-1]), 0, length)
            total = total + dot0(weight[:, i].reshape(-1, lanes), part)
        return total

    mixes = [lax.dynamic_index_in_dim(group_mix[i], col_rank, 0, keepdims=False) for i in range(2)]

    mid_rows = rows + 2 * REACH
    start = row_rank * rows
    branch = mixed_branch(product(w_first, ext_rows), scaling, mixes[0], start - REACH, total_rows, code)
    branch_all = lax.all_gather(branch, "tp", axis=0, tiled=True)
    ahead = product(w_second, block.shape[1])
    joint = lax.all_gather(ahead[:, ext_rows:].astype(bf16).T, "sp", axis=0, tiled=True)
    resid = (window(block, REACH, mid_rows).astype(f32) + dot0(outs[0], branch_all)).astype(bf16)
    resid_f = resid.astype(f32)
    square_sum = sent_to_all(jnp.sum(resid_f * resid_f, axis=0), "tp").sum(axis=0)
    scaling = lax.rsqrt(square_sum / full_width + norm_eps)

    sums = window(ahead, REACH, mid_rows) + dot0(joint, branch_all)
    branch = mixed_branch(sums, scaling, mixes[1], start, total_rows, code)
    chips = tp_size // CORES
    twins = [[CORES * i + c for i in range(chips)] for c in range(CORES)]
    mine = lax.all_gather(branch, "tp", axis=0, tiled=True, axis_index_groups=twins)
    other = swap_cores(mine)
    w_last = outs[1].reshape(chips, CORES, chans, cols)
    own, partner = (
        lax.dynamic_index_in_dim(w_last, c, 1, keepdims=False).reshape(-1, cols) for c in (core, 1 - core)
    )
    resid = window(resid_f, REACH, rows) + dot0(own, mine) + dot0(partner, other)
    return resid.astype(bf16).T


def solution(mesh):
    in_specs = (
        P(("grp", "sp"), "tp"),
        P(),
        P(None, "sp", "tp"),
        P(None, "sp", "tp"),
        P(),
        P(None, "sp", "tp"),
    )
    out_specs = P(("grp", "sp"), "tp")
    return jax.shard_map(local, mesh=mesh, in_specs=in_specs, out_specs=out_specs, check_vma=False)
```

```python
import jax
import jax.numpy as jnp
from jax import lax
from jax.experimental import pallas as pl
from jax.experimental.pallas import tpu as pltpu
from jax.sharding import PartitionSpec as P

GROUP = 64
CORES = 2
REACH = 8
norm_eps = 1e-06
bf16 = jnp.bfloat16
f32 = jnp.float32


def sent_to_all(array, axis):
    copies = jnp.broadcast_to(array, (lax.axis_size(axis), *array.shape))
    return lax.all_to_all(copies, axis, split_axis=0, concat_axis=0, tiled=True)


def swap_cores(array):
    size = lax.axis_size("tp")
    return lax.ppermute(array, "tp", [(i, i ^ 1) for i in range(size)])


def shifted_over_chips(array, step):
    size = lax.axis_size("tp")
    return lax.ppermute(array, "tp", [(i, (i + CORES * step) % size) for i in range(size)])


def same_core_blocks(block):
    chips = lax.axis_size("tp") // CORES
    chip = lax.axis_index("tp") // CORES
    out = jnp.zeros((chips, *block.shape), block.dtype)
    origin = (0,) * block.ndim
    out = lax.dynamic_update_slice(out, block[None], (chip, *origin))
    right = left = block
    for step in range(1, chips // 2 + 1):
        right = shifted_over_chips(right, 1)
        out = lax.dynamic_update_slice(out, right[None], ((chip - step) % chips, *origin))
        if step < chips - chips // 2:
            left = shifted_over_chips(left, -1)
            out = lax.dynamic_update_slice(out, left[None], ((chip + step) % chips, *origin))
    return out


def dot0(left, right):
    return lax.dot_general(left, right, (((0,), (0,)), ((), ())), preferred_element_type=f32)


def window(array, start, length):
    return lax.slice_in_dim(array, start, start + length, axis=1)


def first_kernel(chans, rows, ext_rows, full_width, total_rows, at, mine, other, w_mine, w_other, mix, branch, ahead, joint, acc, squares, turned):
    step = pl.program_id(0)
    depth = mine.shape[2]
    lanes = 2 * chans
    count = mine.shape[1]

    @pl.when(step == 0)
    def _():
        acc[...] = jnp.zeros_like(acc)
        squares[...] = jnp.zeros_like(squares)

    for block, weight in ((mine, w_mine), (other, w_other)):
        part = block[0]
        acc[...] += lax.dot_general(part, weight[0], (((1,), (1,)), ((), ())), preferred_element_type=f32)
        wide = part.astype(f32)
        wide = wide * wide
        total = wide[:, :lanes]
        for i in range(lanes, depth, lanes):
            total = total + wide[:, i : i + lanes]
        squares[...] += total

    @pl.when(step == pl.num_programs(0) - 1)
    def _():
        code = at[1]
        scaling = lax.rsqrt(jnp.sum(squares[...], axis=1, keepdims=True) / full_width + norm_eps)
        both = (acc[:, :lanes] * scaling).astype(bf16).astype(f32)
        running = both
        total = None
        for code_value, size in enumerate((1, 2, 4, 8)):
            running = running + pltpu.roll(running, count - size, 0)
            picked = pltpu.roll(running, size, 0)
            total = picked if total is None else jnp.where(code == code_value, picked, total)
        position = at[2] + lax.broadcasted_iota(jnp.int32, (count, lanes), 0)
        half = jnp.left_shift(1, code)
        counted = jnp.minimum(position + half, total_rows) - jnp.maximum(position - half, 0)
        counted = jnp.maximum(counted, 1).astype(f32)
        pooled = (total / counted - both).astype(bf16)
        mixed = jnp.dot(pooled, mix[...], preferred_element_type=f32)
        gated = mixed * (both / (1.0 + jnp.exp(-both)))
        turned[:count] = pltpu.roll(gated, count - REACH, 0)
        branch[...] = turned[...].T[:chans, :rows].astype(bf16)
        turned[:count] = pltpu.roll(acc[:, lanes:], count - REACH, 0)
        ahead[...] = turned[...].T[:, :rows]
        joint[...] = acc[ext_rows:, lanes:].astype(bf16)


def first_layer(mine, other, gathered, mix, at, chans, ext_rows, full_width, total_rows):
    chips, count, depth = mine.shape
    lanes = 2 * chans
    rows = ext_rows - 2 * REACH
    padded = -(-count // 128) * 128

    def block(step, at):
        return (step, 0, 0)

    return pl.pallas_call(
        lambda *refs: first_kernel(chans, rows, ext_rows, full_width, total_rows, *refs),
        grid_spec=pltpu.PrefetchScalarGridSpec(
            num_scalar_prefetch=1,
            grid=(chips,),
            in_specs=[
                pl.BlockSpec((1, count, depth), block),
                pl.BlockSpec((1, count, depth), block),
                pl.BlockSpec((1, 2 * lanes, depth), lambda step, at: (CORES * step + at[0], 0, 0)),
                pl.BlockSpec((1, 2 * lanes, depth), lambda step, at: (CORES * step + 1 - at[0], 0, 0)),
                pl.BlockSpec((lanes, lanes), lambda step, at: (0, 0)),
            ],
            out_specs=[
                pl.BlockSpec((chans, rows), lambda step, at: (0, 0)),
                pl.BlockSpec((lanes, rows), lambda step, at: (0, 0)),
                pl.BlockSpec((count - ext_rows, lanes), lambda step, at: (0, 0)),
            ],
            scratch_shapes=[
                pltpu.VMEM((count, 2 * lanes), f32),
                pltpu.VMEM((count, lanes), f32),
                pltpu.VMEM((padded, lanes), f32),
            ],
        ),
        out_shape=[
            jax.ShapeDtypeStruct((chans, rows), bf16),
            jax.ShapeDtypeStruct((lanes, rows), f32),
            jax.ShapeDtypeStruct((count - ext_rows, lanes), bf16),
        ],
        compiler_params=pltpu.CompilerParams(dimension_semantics=("arbitrary",)),
        cost_estimate=pl.CostEstimate(
            flops=CORES * chips * count * depth * 4 * lanes,
            bytes_accessed=CORES * chips * depth * 2 * (count + 2 * lanes),
            transcendentals=0,
        ),
        name="first_layer",
    )(at, mine, other, gathered, gathered, mix)


def mixed_branch(sums, scaling, mix, first_position, total_rows, code):
    rows = sums.shape[1] - 2 * REACH
    chans = sums.shape[0] // 2
    scaled = (sums * scaling[None, :]).astype(bf16).astype(f32)
    pool_in = scaled[chans:]
    gate = window(scaled[:chans], REACH, rows)
    position = first_position + jnp.arange(rows, dtype=jnp.int32)
    half = jnp.left_shift(1, code)
    counted = jnp.minimum(position + half, total_rows) - jnp.maximum(position - half, 0)
    counted = counted.astype(f32)
    running = pool_in
    total = None
    for code_value, size in enumerate((1, 2, 4, 8)):
        width = running.shape[1] - size
        running = window(running, 0, width) + window(running, size, width)
        picked = window(running, REACH - size, rows)
        total = picked if total is None else jnp.where(code == code_value, picked, total)
    pooled = (total / counted[None, :] - window(pool_in, REACH, rows)).astype(bf16)
    mixed = dot0(mix, pooled)
    return (mixed * jax.nn.silu(gate)).astype(bf16)


def local(hidden_in, norm_gain, w_pool_in, w_pool_gate, group_mix, w_out):
    rows, cols = hidden_in.shape
    chans = w_pool_in.shape[2]
    depth = w_pool_in.shape[1]
    out_rows = w_out.shape[1]
    col_rank = lax.axis_index("tp")
    row_rank = lax.axis_index("sp")
    tp_size = lax.axis_size("tp")
    sp_size = lax.axis_size("sp")
    chips = tp_size // CORES
    core = jnp.bitwise_and(col_rank, CORES - 1)
    total_rows = rows * sp_size
    full_width = cols * tp_size
    code = jnp.bitwise_and(col_rank, 3)
    halo = 2 * REACH
    ext_rows = rows + 2 * halo
    lanes = 2 * chans

    packed = []
    for layer in range(2):
        gain = lax.dynamic_slice_in_dim(norm_gain[layer], row_rank * depth, depth)[None, :]
        both = jnp.concatenate([w_pool_gate[layer].T, w_pool_in[layer].T], axis=0)
        packed.append((both.astype(f32) * gain).astype(bf16))
    packed = jnp.concatenate([*packed, w_out[0], w_out[1]], axis=0)
    packed, hidden_in = lax.optimization_barrier((packed, hidden_in))
    gathered = lax.all_gather(packed, "sp", axis=0, tiled=False)
    at = 2 * lanes
    outs = [
        gathered[:, at + i * out_rows : at + (i + 1) * out_rows].reshape(chips, CORES * out_rows, cols)
        for i in range(2)
    ]

    up = [(i, i + 1) for i in range(sp_size - 1)]
    down = [(j, i) for i, j in up]
    before = lax.ppermute(hidden_in[rows - halo :], "sp", up)
    after = lax.ppermute(hidden_in[:halo], "sp", down)
    block = jnp.concatenate([before, hidden_in, after, w_out[0]], axis=0)
    mine = same_core_blocks(block)
    other = swap_cores(mine)

    def by_core(array):
        size = array.shape[1] // CORES
        return [
            lax.dynamic_slice_in_dim(array, c * size, size, axis=1).reshape(-1, array.shape[2]) for c in (core, 1 - core)
        ]

    twins = [[CORES * i + c for i in range(chips)] for c in range(CORES)]

    def gathered_branch(branch):
        same = lax.all_gather(branch, "tp", axis=0, tiled=True, axis_index_groups=twins)
        return same, swap_cores(same)

    def product(weights, operands):
        return sum(dot0(weight, operand) for weight, operand in zip(weights, operands))

    mixes = [lax.dynamic_index_in_dim(group_mix[i], col_rank, 0, keepdims=False) for i in range(2)]

    mid_rows = rows + 2 * REACH
    start = row_rank * rows
    mix = jnp.pad(mixes[0], ((chans, 0), (0, chans)))
    scalars = jnp.stack([core, code, start - halo]).astype(jnp.int32)
    branch, ahead, joint = first_layer(mine, other, gathered, mix, scalars, chans, ext_rows, full_width, total_rows)
    joint = sent_to_all(joint, "sp").reshape(chips, CORES * out_rows, lanes)
    pair = gathered_branch(branch)
    resid = (block[REACH : REACH + mid_rows].T.astype(f32) + product(by_core(outs[0]), pair)).astype(bf16)
    resid_f = resid.astype(f32)
    square_sum = sent_to_all(jnp.sum(resid_f * resid_f, axis=0), "tp").sum(axis=0)
    scaling = lax.rsqrt(square_sum / full_width + norm_eps)

    sums = ahead + product(by_core(joint), pair)
    branch = mixed_branch(sums, scaling, mixes[1], start, total_rows, code)
    pair = gathered_branch(branch)
    resid = window(resid_f, REACH, rows) + product(by_core(outs[1]), pair)
    return resid.astype(bf16).T


def solution(mesh):
    in_specs = (
        P(("grp", "sp"), "tp"),
        P(),
        P(None, "sp", "tp"),
        P(None, "sp", "tp"),
        P(),
        P(None, "sp", "tp"),
    )
    out_specs = P(("grp", "sp"), "tp")
    return jax.shard_map(local, mesh=mesh, in_specs=in_specs, out_specs=out_specs, check_vma=False)
```

```python
import jax
import jax.numpy as jnp
from jax import lax
from jax.experimental import pallas as pl
from jax.experimental.pallas import tpu as pltpu
from jax.sharding import PartitionSpec as P

GROUP = 64
CORES = 2
REACH = 8
PAIR = 2
norm_eps = 1e-06
bf16 = jnp.bfloat16
f32 = jnp.float32


def sent_to_all(array, axis):
    copies = jnp.broadcast_to(array, (lax.axis_size(axis), *array.shape))
    return lax.all_to_all(copies, axis, split_axis=0, concat_axis=0, tiled=True)


def swap_cores(array):
    size = lax.axis_size("tp")
    return lax.ppermute(array, "tp", [(i, i ^ 1) for i in range(size)])


def shifted_over_chips(array, step):
    size = lax.axis_size("tp")
    return lax.ppermute(array, "tp", [(i, (i + CORES * step) % size) for i in range(size)])


def same_core_blocks(block):
    chips = lax.axis_size("tp") // CORES
    chip = lax.axis_index("tp") // CORES
    out = jnp.zeros((chips, *block.shape), block.dtype)
    origin = (0,) * block.ndim
    out = lax.dynamic_update_slice(out, block[None], (chip, *origin))
    right = left = block
    for step in range(1, chips // 2 + 1):
        right = shifted_over_chips(right, 1)
        out = lax.dynamic_update_slice(out, right[None], ((chip - step) % chips, *origin))
        if step < chips - chips // 2:
            left = shifted_over_chips(left, -1)
            out = lax.dynamic_update_slice(out, left[None], ((chip + step) % chips, *origin))
    return out


def dot0(left, right):
    return lax.dot_general(left, right, (((0,), (0,)), ((), ())), preferred_element_type=f32)


def window(array, start, length):
    return lax.slice_in_dim(array, start, start + length, axis=1)


def squares_kernel(full_width, mine, other, scaling, squares):
    step = pl.program_id(0)
    lanes = squares.shape[1]

    @pl.when(step == 0)
    def _():
        squares[...] = jnp.zeros_like(squares)

    total = squares[...]
    for block in (mine, other):
        for chip in range(block.shape[0]):
            for i in range(0, block.shape[2], lanes):
                part = block[chip, :, i : i + lanes].astype(f32)
                total = total + part * part
    squares[...] = total

    @pl.when(step == pl.num_programs(0) - 1)
    def _():
        mean = jnp.sum(squares[...], axis=1, keepdims=True) / full_width
        scaling[...] = jnp.broadcast_to(lax.rsqrt(mean + norm_eps), scaling.shape)


def row_scaling(mine, other, full_width):
    chips, count, depth = mine.shape
    spec = pl.BlockSpec((PAIR, count, depth), lambda step: (step, 0, 0))
    return pl.pallas_call(
        lambda *refs: squares_kernel(full_width, *refs),
        grid=(chips // PAIR,),
        in_specs=[spec, spec],
        out_specs=pl.BlockSpec((count, 128), lambda step: (0, 0)),
        scratch_shapes=[pltpu.VMEM((count, 128), f32)],
        out_shape=jax.ShapeDtypeStruct((count, 128), f32),
        compiler_params=pltpu.CompilerParams(dimension_semantics=("arbitrary",)),
        cost_estimate=pl.CostEstimate(
            flops=4 * CORES * chips * count * depth, bytes_accessed=CORES * chips * count * depth * 2, transcendentals=0
        ),
        name="row_scaling",
    )(mine, other)


def first_kernel(chans, rows, ext_rows, total_rows, at, mine, other, scaling, w_all, mix, branch, ahead, joint, acc, turned):
    step = pl.program_id(0)
    lanes = 2 * chans
    count = mine.shape[1]
    core = at[0]
    total = 0
    for chip in range(mine.shape[0]):
        for block, place in ((mine, core), (other, 1 - core)):
            weight = w_all[CORES * chip + place]
            total = total + lax.dot_general(
                block[chip], weight, (((1,), (1,)), ((), ())), preferred_element_type=f32
            )

    @pl.when(step == 0)
    def _():
        acc[...] = total

    @pl.when(step > 0)
    def _():
        acc[...] += total

    @pl.when(step == pl.num_programs(0) - 1)
    def _():
        code = at[1]
        both = (acc[:, :lanes] * scaling[...]).astype(bf16).astype(f32)
        running = both
        total = None
        for code_value, size in enumerate((1, 2, 4, 8)):
            running = running + pltpu.roll(running, count - size, 0)
            picked = pltpu.roll(running, size, 0)
            total = picked if total is None else jnp.where(code == code_value, picked, total)
        position = at[2] + lax.broadcasted_iota(jnp.int32, (count, lanes), 0)
        half = jnp.left_shift(1, code)
        counted = jnp.minimum(position + half, total_rows) - jnp.maximum(position - half, 0)
        counted = jnp.maximum(counted, 1).astype(f32)
        pooled = (total / counted - both).astype(bf16)
        mixed = jnp.dot(pooled, mix[...], preferred_element_type=f32)
        gated = mixed * (both / (1.0 + jnp.exp(-both)))
        turned[:count] = pltpu.roll(gated, count - REACH, 0)
        branch[...] = turned[...].T[:chans, :rows].astype(bf16)
        turned[:count] = pltpu.roll(acc[:, lanes:], count - REACH, 0)
        ahead[...] = turned[...].T[:, :rows]
        joint[...] = acc[ext_rows:, lanes:].astype(bf16)


def first_layer(mine, other, scaling, gathered, mix, at, chans, ext_rows, total_rows):
    chips, count, depth = mine.shape
    lanes = 2 * chans
    rows = ext_rows - 2 * REACH
    padded = -(-count // 128) * 128

    def block(step, at):
        return (step, 0, 0)

    def whole(step, at):
        return (0, 0)

    return pl.pallas_call(
        lambda *refs: first_kernel(chans, rows, ext_rows, total_rows, *refs),
        grid_spec=pltpu.PrefetchScalarGridSpec(
            num_scalar_prefetch=1,
            grid=(chips // PAIR,),
            in_specs=[
                pl.BlockSpec((PAIR, count, depth), block),
                pl.BlockSpec((PAIR, count, depth), block),
                pl.BlockSpec((count, lanes), whole),
                pl.BlockSpec((CORES * PAIR, 2 * lanes, depth), block),
                pl.BlockSpec((lanes, lanes), whole),
            ],
            out_specs=[
                pl.BlockSpec((chans, rows), whole),
                pl.BlockSpec((lanes, rows), whole),
                pl.BlockSpec((count - ext_rows, lanes), whole),
            ],
            scratch_shapes=[
                pltpu.VMEM((count, 2 * lanes), f32),
                pltpu.VMEM((padded, lanes), f32),
            ],
        ),
        out_shape=[
            jax.ShapeDtypeStruct((chans, rows), bf16),
            jax.ShapeDtypeStruct((lanes, rows), f32),
            jax.ShapeDtypeStruct((count - ext_rows, lanes), bf16),
        ],
        compiler_params=pltpu.CompilerParams(dimension_semantics=("arbitrary",)),
        cost_estimate=pl.CostEstimate(
            flops=CORES * chips * count * depth * 4 * lanes,
            bytes_accessed=CORES * chips * depth * 2 * (count + 2 * lanes),
            transcendentals=0,
        ),
        name="first_layer",
    )(at, mine, other, scaling, gathered, mix)


def mixed_branch(sums, scaling, mix, first_position, total_rows, code):
    rows = sums.shape[1] - 2 * REACH
    chans = sums.shape[0] // 2
    scaled = (sums * scaling[None, :]).astype(bf16).astype(f32)
    pool_in = scaled[chans:]
    gate = window(scaled[:chans], REACH, rows)
    position = first_position + jnp.arange(rows, dtype=jnp.int32)
    half = jnp.left_shift(1, code)
    counted = jnp.minimum(position + half, total_rows) - jnp.maximum(position - half, 0)
    counted = counted.astype(f32)
    running = pool_in
    total = None
    for code_value, size in enumerate((1, 2, 4, 8)):
        width = running.shape[1] - size
        running = window(running, 0, width) + window(running, size, width)
        picked = window(running, REACH - size, rows)
        total = picked if total is None else jnp.where(code == code_value, picked, total)
    pooled = (total / counted[None, :] - window(pool_in, REACH, rows)).astype(bf16)
    mixed = dot0(mix, pooled)
    return (mixed * jax.nn.silu(gate)).astype(bf16)


def local(hidden_in, norm_gain, w_pool_in, w_pool_gate, group_mix, w_out):
    rows, cols = hidden_in.shape
    chans = w_pool_in.shape[2]
    depth = w_pool_in.shape[1]
    out_rows = w_out.shape[1]
    col_rank = lax.axis_index("tp")
    row_rank = lax.axis_index("sp")
    tp_size = lax.axis_size("tp")
    sp_size = lax.axis_size("sp")
    chips = tp_size // CORES
    core = jnp.bitwise_and(col_rank, CORES - 1)
    total_rows = rows * sp_size
    full_width = cols * tp_size
    code = jnp.bitwise_and(col_rank, 3)
    halo = 2 * REACH
    ext_rows = rows + 2 * halo
    lanes = 2 * chans

    packed = []
    for layer in range(2):
        gain = lax.dynamic_slice_in_dim(norm_gain[layer], row_rank * depth, depth)[None, :]
        both = jnp.concatenate([w_pool_gate[layer].T, w_pool_in[layer].T], axis=0)
        packed.append((both.astype(f32) * gain).astype(bf16))
    packed = jnp.concatenate([*packed, w_out[0], w_out[1]], axis=0)
    packed, hidden_in = lax.optimization_barrier((packed, hidden_in))
    gathered = lax.all_gather(packed, "sp", axis=0, tiled=False)
    at = 2 * lanes
    outs = [
        gathered[:, at + i * out_rows : at + (i + 1) * out_rows].reshape(chips, CORES * out_rows, cols)
        for i in range(2)
    ]

    up = [(i, i + 1) for i in range(sp_size - 1)]
    down = [(j, i) for i, j in up]
    before = lax.ppermute(hidden_in[rows - halo :], "sp", up)
    after = lax.ppermute(hidden_in[:halo], "sp", down)
    block = jnp.concatenate([before, hidden_in, after, w_out[0]], axis=0)
    mine = same_core_blocks(block)
    other = swap_cores(mine)

    def by_core(array):
        size = array.shape[1] // CORES
        return [
            lax.dynamic_slice_in_dim(array, c * size, size, axis=1).reshape(-1, array.shape[2]) for c in (core, 1 - core)
        ]

    twins = [[CORES * i + c for i in range(chips)] for c in range(CORES)]

    def over_twins(branch):
        return lax.all_gather(branch, "tp", axis=0, tiled=True, axis_index_groups=twins)

    def product(weights, operands):
        return sum(dot0(weight, operand) for weight, operand in zip(weights, operands))

    mixes = [lax.dynamic_index_in_dim(group_mix[i], col_rank, 0, keepdims=False) for i in range(2)]

    mid_rows = rows + 2 * REACH
    start = row_rank * rows
    mix = jnp.pad(mixes[0], ((chans, 0), (0, chans)))
    scalars = jnp.stack([core, code, start - halo]).astype(jnp.int32)
    scaling = row_scaling(mine, other, full_width)
    branch, ahead, joint = first_layer(mine, other, scaling, gathered, mix, scalars, chans, ext_rows, total_rows)
    joint = sent_to_all(joint, "sp")
    same = over_twins(branch)
    same, joint = lax.optimization_barrier((same, joint))
    joint = joint.reshape(chips, CORES * out_rows, lanes)
    pair = same, swap_cores(same)
    resid = (block[REACH : REACH + mid_rows].T.astype(f32) + product(by_core(outs[0]), pair)).astype(bf16)
    resid_f = resid.astype(f32)
    square_sum = sent_to_all(jnp.sum(resid_f * resid_f, axis=0), "tp").sum(axis=0)
    scaling = lax.rsqrt(square_sum / full_width + norm_eps)

    sums = ahead + product(by_core(joint), pair)
    branch = mixed_branch(sums, scaling, mixes[1], start, total_rows, code)
    same = over_twins(branch)
    pair = same, swap_cores(same)
    resid = window(resid_f, REACH, rows) + product(by_core(outs[1]), pair)
    return resid.astype(bf16).T


def solution(mesh):
    in_specs = (
        P(("grp", "sp"), "tp"),
        P(),
        P(None, "sp", "tp"),
        P(None, "sp", "tp"),
        P(),
        P(None, "sp", "tp"),
    )
    out_specs = P(("grp", "sp"), "tp")
    return jax.shard_map(local, mesh=mesh, in_specs=in_specs, out_specs=out_specs, check_vma=False)
```

```python
import jax
import jax.numpy as jnp
from jax import lax
from jax.experimental import pallas as pl
from jax.experimental.pallas import tpu as pltpu
from jax.sharding import PartitionSpec as P

GROUP = 64
CORES = 2
REACH = 8
PAIR = 4
norm_eps = 1e-06
bf16 = jnp.bfloat16
f32 = jnp.float32


def sent_to_all(array, axis):
    copies = jnp.broadcast_to(array, (lax.axis_size(axis), *array.shape))
    return lax.all_to_all(copies, axis, split_axis=0, concat_axis=0, tiled=True)


def swap_cores(array):
    size = lax.axis_size("tp")
    return lax.ppermute(array, "tp", [(i, i ^ 1) for i in range(size)])


def shifted_over_chips(array, step):
    size = lax.axis_size("tp")
    return lax.ppermute(array, "tp", [(i, (i + CORES * step) % size) for i in range(size)])


def same_core_blocks(block):
    chips = lax.axis_size("tp") // CORES
    chip = lax.axis_index("tp") // CORES
    out = jnp.zeros((chips, *block.shape), block.dtype)
    origin = (0,) * block.ndim
    out = lax.dynamic_update_slice(out, block[None], (chip, *origin))
    right = left = block
    for step in range(1, chips // 2 + 1):
        right = shifted_over_chips(right, 1)
        out = lax.dynamic_update_slice(out, right[None], ((chip - step) % chips, *origin))
        if step < chips - chips // 2:
            left = shifted_over_chips(left, -1)
            out = lax.dynamic_update_slice(out, left[None], ((chip + step) % chips, *origin))
    return out


def dot0(left, right):
    return lax.dot_general(left, right, (((0,), (0,)), ((), ())), preferred_element_type=f32)


def window(array, start, length):
    return lax.slice_in_dim(array, start, start + length, axis=1)


def pack_kernel(at, w_gate, w_in, w_last, gain, packed):
    layers, chans, _ = w_gate.shape
    rows = 0
    for layer in range(layers):
        for weight in (w_gate, w_in):
            packed[rows : rows + chans] = (weight[layer].astype(f32) * gain[layer : layer + 1]).astype(bf16)
            rows += chans
    for layer in range(layers):
        packed[rows : rows + w_last.shape[1]] = w_last[layer]
        rows += w_last.shape[1]


def packed_weights(w_gate, w_in, w_last, gain, row_rank):
    layers, chans, depth = w_gate.shape
    rows = layers * (2 * chans + w_last.shape[1])

    def whole(array):
        return pl.BlockSpec(array.shape, lambda step, at: (0, 0, 0))

    return pl.pallas_call(
        pack_kernel,
        grid_spec=pltpu.PrefetchScalarGridSpec(
            num_scalar_prefetch=1,
            grid=(1,),
            in_specs=[
                whole(w_gate),
                whole(w_in),
                whole(w_last),
                pl.BlockSpec((layers, depth), lambda step, at: (0, at[0])),
            ],
            out_specs=pl.BlockSpec((rows, depth), lambda step, at: (0, 0)),
        ),
        out_shape=jax.ShapeDtypeStruct((rows, depth), bf16),
        name="packed_weights",
    )(row_rank.reshape(1).astype(jnp.int32), w_gate, w_in, w_last, gain)


def squares_kernel(full_width, mine, other, scaling, squares):
    step = pl.program_id(0)
    lanes = squares.shape[1]

    @pl.when(step == 0)
    def _():
        squares[...] = jnp.zeros_like(squares)

    total = squares[...]
    for block, first in ((mine, PAIR * step), (other, 0)):
        for chip in range(PAIR):
            for i in range(0, block.shape[2], lanes):
                part = block[first + chip, :, i : i + lanes].astype(f32)
                total = total + part * part
    squares[...] = total

    @pl.when(step == pl.num_programs(0) - 1)
    def _():
        mean = jnp.sum(squares[...], axis=1, keepdims=True) / full_width
        scaling[...] = jnp.broadcast_to(lax.rsqrt(mean + norm_eps), scaling.shape)


def row_scaling(mine, other, full_width):
    chips, count, depth = mine.shape
    specs = [pl.BlockSpec(memory_space=pltpu.VMEM), pl.BlockSpec((PAIR, count, depth), lambda step: (step, 0, 0))]
    return pl.pallas_call(
        lambda *refs: squares_kernel(full_width, *refs),
        grid=(chips // PAIR,),
        in_specs=specs,
        out_specs=pl.BlockSpec((count, 128), lambda step: (0, 0)),
        scratch_shapes=[pltpu.VMEM((count, 128), f32)],
        out_shape=jax.ShapeDtypeStruct((count, 128), f32),
        compiler_params=pltpu.CompilerParams(dimension_semantics=("arbitrary",), vmem_limit_bytes=28 << 20),
        cost_estimate=pl.CostEstimate(
            flops=4 * CORES * chips * count * depth, bytes_accessed=CORES * chips * count * depth * 2, transcendentals=0
        ),
        name="row_scaling",
    )(mine, other)


def first_kernel(chans, rows, ext_rows, total_rows, at, mine, other, scaling, w_all, mix, branch, ahead, joint, acc, turned):
    step = pl.program_id(0)
    lanes = 2 * chans
    count = mine.shape[1]
    core = at[0]
    total = 0
    for chip in range(PAIR):
        for part, place in ((mine[PAIR * step + chip], core), (other[chip], 1 - core)):
            weight = w_all[CORES * chip + place]
            total = total + lax.dot_general(
                part, weight, (((1,), (1,)), ((), ())), preferred_element_type=f32
            )

    @pl.when(step == 0)
    def _():
        acc[...] = total

    @pl.when(step > 0)
    def _():
        acc[...] += total

    @pl.when(step == pl.num_programs(0) - 1)
    def _():
        code = at[1]
        both = (acc[:, :lanes] * scaling[...]).astype(bf16).astype(f32)
        running = both
        total = None
        for code_value, size in enumerate((1, 2, 4, 8)):
            running = running + pltpu.roll(running, count - size, 0)
            picked = pltpu.roll(running, size, 0)
            total = picked if total is None else jnp.where(code == code_value, picked, total)
        position = at[2] + lax.broadcasted_iota(jnp.int32, (count, lanes), 0)
        half = jnp.left_shift(1, code)
        counted = jnp.minimum(position + half, total_rows) - jnp.maximum(position - half, 0)
        counted = jnp.maximum(counted, 1).astype(f32)
        pooled = (total / counted - both).astype(bf16)
        mixed = jnp.dot(pooled, mix[...], preferred_element_type=f32)
        gated = mixed * (both / (1.0 + jnp.exp(-both)))
        turned[:count] = pltpu.roll(gated, count - REACH, 0)
        branch[...] = turned[...].T[:chans, :rows].astype(bf16)
        turned[:count] = pltpu.roll(acc[:, lanes:], count - REACH, 0)
        ahead[...] = turned[...].T[:, :rows]
        joint[...] = acc[ext_rows:, lanes:].astype(bf16)


def first_layer(mine, other, scaling, gathered, mix, at, chans, ext_rows, total_rows):
    chips, count, depth = mine.shape
    lanes = 2 * chans
    rows = ext_rows - 2 * REACH
    padded = -(-count // 128) * 128

    def block(step, at):
        return (step, 0, 0)

    def whole(step, at):
        return (0, 0)

    return pl.pallas_call(
        lambda *refs: first_kernel(chans, rows, ext_rows, total_rows, *refs),
        grid_spec=pltpu.PrefetchScalarGridSpec(
            num_scalar_prefetch=1,
            grid=(chips // PAIR,),
            in_specs=[
                pl.BlockSpec(memory_space=pltpu.VMEM),
                pl.BlockSpec((PAIR, count, depth), block),
                pl.BlockSpec((count, lanes), whole),
                pl.BlockSpec((CORES * PAIR, 2 * lanes, depth), block),
                pl.BlockSpec((lanes, lanes), whole),
            ],
            out_specs=[
                pl.BlockSpec((chans, rows), whole),
                pl.BlockSpec((lanes, rows), whole),
                pl.BlockSpec((count - ext_rows, lanes), whole),
            ],
            scratch_shapes=[
                pltpu.VMEM((count, 2 * lanes), f32),
                pltpu.VMEM((padded, lanes), f32),
            ],
        ),
        out_shape=[
            jax.ShapeDtypeStruct((chans, rows), bf16),
            jax.ShapeDtypeStruct((lanes, rows), f32),
            jax.ShapeDtypeStruct((count - ext_rows, lanes), bf16),
        ],
        compiler_params=pltpu.CompilerParams(dimension_semantics=("arbitrary",), vmem_limit_bytes=28 << 20),
        cost_estimate=pl.CostEstimate(
            flops=CORES * chips * count * depth * 4 * lanes,
            bytes_accessed=CORES * chips * depth * 2 * (count + 2 * lanes),
            transcendentals=0,
        ),
        name="first_layer",
    )(at, mine, other, scaling, gathered, mix)


def mixed_branch(sums, scaling, mix, first_position, total_rows, code):
    rows = sums.shape[1] - 2 * REACH
    chans = sums.shape[0] // 2
    scaled = (sums * scaling[None, :]).astype(bf16).astype(f32)
    pool_in = scaled[chans:]
    gate = window(scaled[:chans], REACH, rows)
    position = first_position + jnp.arange(rows, dtype=jnp.int32)
    half = jnp.left_shift(1, code)
    counted = jnp.minimum(position + half, total_rows) - jnp.maximum(position - half, 0)
    counted = counted.astype(f32)
    running = pool_in
    total = None
    for code_value, size in enumerate((1, 2, 4, 8)):
        width = running.shape[1] - size
        running = window(running, 0, width) + window(running, size, width)
        picked = window(running, REACH - size, rows)
        total = picked if total is None else jnp.where(code == code_value, picked, total)
    pooled = (total / counted[None, :] - window(pool_in, REACH, rows)).astype(bf16)
    mixed = dot0(mix, pooled)
    return (mixed * jax.nn.silu(gate)).astype(bf16)


def local(hidden_in, norm_gain, w_pool_in, w_pool_gate, group_mix, w_out):
    rows, cols = hidden_in.shape
    chans = w_pool_in.shape[2]
    depth = w_pool_in.shape[1]
    out_rows = w_out.shape[1]
    col_rank = lax.axis_index("tp")
    row_rank = lax.axis_index("sp")
    tp_size = lax.axis_size("tp")
    sp_size = lax.axis_size("sp")
    chips = tp_size // CORES
    core = jnp.bitwise_and(col_rank, CORES - 1)
    total_rows = rows * sp_size
    full_width = cols * tp_size
    code = jnp.bitwise_and(col_rank, 3)
    halo = 2 * REACH
    ext_rows = rows + 2 * halo
    lanes = 2 * chans

    packed = packed_weights(w_pool_gate.transpose(0, 2, 1), w_pool_in.transpose(0, 2, 1), w_out, norm_gain, row_rank)
    packed, hidden_in = lax.optimization_barrier((packed, hidden_in))
    gathered = lax.all_gather(packed, "sp", axis=0, tiled=False)

    def last_rows(gathered, layer):
        at = 2 * lanes + layer * out_rows
        return gathered[:, at : at + out_rows].reshape(chips, CORES * out_rows, cols)

    up = [(i, i + 1) for i in range(sp_size - 1)]
    down = [(j, i) for i, j in up]
    before = lax.ppermute(hidden_in[rows - halo :], "sp", up)
    after = lax.ppermute(hidden_in[:halo], "sp", down)
    block = jnp.concatenate([before, hidden_in, after, w_out[0]], axis=0)
    mine = same_core_blocks(block)
    other = swap_cores(mine)

    def by_core(array):
        size = array.shape[1] // CORES
        return [
            lax.dynamic_slice_in_dim(array, c * size, size, axis=1).reshape(-1, array.shape[2]) for c in (core, 1 - core)
        ]

    twins = [[CORES * i + c for i in range(chips)] for c in range(CORES)]

    def over_twins(branch):
        return lax.all_gather(branch, "tp", axis=0, tiled=True, axis_index_groups=twins)

    def product(weights, operands):
        return sum(dot0(weight, operand) for weight, operand in zip(weights, operands))

    mixes = [lax.dynamic_index_in_dim(group_mix[i], col_rank, 0, keepdims=False) for i in range(2)]

    mid_rows = rows + 2 * REACH
    start = row_rank * rows
    mix = jnp.pad(mixes[0], ((chans, 0), (0, chans)))
    scalars = jnp.stack([core, code, start - halo]).astype(jnp.int32)
    scaling = row_scaling(mine, other, full_width)
    branch, ahead, joint = first_layer(mine, other, scaling, gathered, mix, scalars, chans, ext_rows, total_rows)
    joint = sent_to_all(joint, "sp")
    same = over_twins(branch)
    same, joint, gathered = lax.optimization_barrier((same, joint, gathered))
    joint = joint.reshape(chips, CORES * out_rows, lanes)
    pair = same, swap_cores(same)
    resid = (block[REACH : REACH + mid_rows].T.astype(f32) + product(by_core(last_rows(gathered, 0)), pair)).astype(bf16)
    resid_f = resid.astype(f32)
    square_sum = sent_to_all(jnp.sum(resid_f * resid_f, axis=0), "tp").sum(axis=0)
    scaling = lax.rsqrt(square_sum / full_width + norm_eps)

    sums = ahead + product(by_core(joint), pair)
    branch = mixed_branch(sums, scaling, mixes[1], start, total_rows, code)
    same = over_twins(branch)
    pair = same, swap_cores(same)
    resid = window(resid_f, REACH, rows) + product(by_core(last_rows(gathered, 1)), pair)
    return resid.astype(bf16).T


def solution(mesh):
    in_specs = (
        P(("grp", "sp"), "tp"),
        P(),
        P(None, "sp", "tp"),
        P(None, "sp", "tp"),
        P(),
        P(None, "sp", "tp"),
    )
    out_specs = P(("grp", "sp"), "tp")
    return jax.shard_map(local, mesh=mesh, in_specs=in_specs, out_specs=out_specs, check_vma=False)
```

```python
import jax
import jax.numpy as jnp
from jax import lax
from jax.experimental import pallas as pl
from jax.experimental.pallas import tpu as pltpu
from jax.sharding import PartitionSpec as P

GROUP = 64
CORES = 2
REACH = 8
PAIR = 4
BLOCKING = 48
norm_eps = 1e-06
bf16 = jnp.bfloat16
f32 = jnp.float32


def sent_to_all(array, axis):
    copies = jnp.broadcast_to(array, (lax.axis_size(axis), *array.shape))
    return lax.all_to_all(copies, axis, split_axis=0, concat_axis=0, tiled=True)


def exchanged(copies, axis):
    return lax.all_to_all(copies, axis, split_axis=0, concat_axis=0, tiled=True)


def swap_cores(array):
    size = lax.axis_size("tp")
    return lax.ppermute(array, "tp", [(i, i ^ 1) for i in range(size)])


def shifted_over_chips(array, step):
    size = lax.axis_size("tp")
    return lax.ppermute(array, "tp", [(i, (i + CORES * step) % size) for i in range(size)])


def same_core_blocks(block):
    chips = lax.axis_size("tp") // CORES
    chip = lax.axis_index("tp") // CORES
    out = jnp.zeros((chips, *block.shape), block.dtype)
    origin = (0,) * block.ndim
    out = lax.dynamic_update_slice(out, block[None], (chip, *origin))
    right = left = block
    for step in range(1, chips // 2 + 1):
        right = shifted_over_chips(right, 1)
        out = lax.dynamic_update_slice(out, right[None], ((chip - step) % chips, *origin))
        if step < chips - chips // 2:
            left = shifted_over_chips(left, -1)
            out = lax.dynamic_update_slice(out, left[None], ((chip + step) % chips, *origin))
    return out


def dot0(left, right):
    return lax.dot_general(left, right, (((0,), (0,)), ((), ())), preferred_element_type=f32)


def window(array, start, length):
    return lax.slice_in_dim(array, start, start + length, axis=1)


def pack_kernel(at, w_gate, w_in, w_last, gain, packed):
    layers, chans, _ = w_gate.shape
    rows = 0
    for layer in range(layers):
        for weight in (w_gate, w_in):
            packed[rows : rows + chans] = (weight[layer].astype(f32) * gain[layer : layer + 1]).astype(bf16)
            rows += chans
    for layer in range(layers):
        packed[rows : rows + w_last.shape[1]] = w_last[layer]
        rows += w_last.shape[1]


def packed_weights(w_gate, w_in, w_last, gain, row_rank):
    layers, chans, depth = w_gate.shape
    rows = layers * (2 * chans + w_last.shape[1])

    def whole(array):
        return pl.BlockSpec(array.shape, lambda step, at: (0, 0, 0))

    return pl.pallas_call(
        pack_kernel,
        grid_spec=pltpu.PrefetchScalarGridSpec(
            num_scalar_prefetch=1,
            grid=(1,),
            in_specs=[
                whole(w_gate),
                whole(w_in),
                whole(w_last),
                pl.BlockSpec((layers, depth), lambda step, at: (0, at[0])),
            ],
            out_specs=pl.BlockSpec((rows, depth), lambda step, at: (0, 0)),
        ),
        out_shape=jax.ShapeDtypeStruct((rows, depth), bf16),
        name="packed_weights",
    )(row_rank.reshape(1).astype(jnp.int32), w_gate, w_in, w_last, gain)


def squares_kernel(full_width, mine, other, scaling, squares):
    step = pl.program_id(0)
    lanes = squares.shape[1]

    @pl.when(step == 0)
    def _():
        squares[...] = jnp.zeros_like(squares)

    total = squares[...]
    for block, first in ((mine, PAIR * step), (other, 0)):
        for chip in range(PAIR):
            for i in range(0, block.shape[2], lanes):
                part = block[first + chip, :, i : i + lanes].astype(f32)
                total = total + part * part
    squares[...] = total

    @pl.when(step == pl.num_programs(0) - 1)
    def _():
        mean = jnp.sum(squares[...], axis=1, keepdims=True) / full_width
        scaling[...] = jnp.broadcast_to(lax.rsqrt(mean + norm_eps), scaling.shape)


def row_scaling(mine, other, full_width):
    chips, count, depth = mine.shape
    specs = [pl.BlockSpec(memory_space=pltpu.VMEM), pl.BlockSpec((PAIR, count, depth), lambda step: (step, 0, 0))]
    return pl.pallas_call(
        lambda *refs: squares_kernel(full_width, *refs),
        grid=(chips // PAIR,),
        in_specs=specs,
        out_specs=pl.BlockSpec((count, 128), lambda step: (0, 0)),
        scratch_shapes=[pltpu.VMEM((count, 128), f32)],
        out_shape=jax.ShapeDtypeStruct((count, 128), f32),
        compiler_params=pltpu.CompilerParams(dimension_semantics=("arbitrary",), vmem_limit_bytes=28 << 20),
        cost_estimate=pl.CostEstimate(
            flops=4 * CORES * chips * count * depth, bytes_accessed=CORES * chips * count * depth * 2, transcendentals=0
        ),
        name="row_scaling",
    )(mine, other)


def first_kernel(chans, rows, ext_rows, total_rows, at, mine, other, scaling, w_all, mix, branch, ahead, joint, acc, turned):
    step = pl.program_id(0)
    lanes = 2 * chans
    count = mine.shape[1]
    core = at[0]
    total = 0
    for chip in range(PAIR):
        for part, place in ((mine[PAIR * step + chip], core), (other[chip], 1 - core)):
            weight = w_all[CORES * chip + place]
            total = total + lax.dot_general(
                part, weight, (((1,), (1,)), ((), ())), preferred_element_type=f32
            )

    @pl.when(step == 0)
    def _():
        acc[...] = total

    @pl.when(step > 0)
    def _():
        acc[...] += total

    @pl.when(step == pl.num_programs(0) - 1)
    def _():
        code = at[1]
        both = (acc[:, :lanes] * scaling[...]).astype(bf16).astype(f32)
        running = both
        total = None
        for code_value, size in enumerate((1, 2, 4, 8)):
            running = running + pltpu.roll(running, count - size, 0)
            picked = pltpu.roll(running, size, 0)
            total = picked if total is None else jnp.where(code == code_value, picked, total)
        position = at[2] + lax.broadcasted_iota(jnp.int32, (count, lanes), 0)
        half = jnp.left_shift(1, code)
        counted = jnp.minimum(position + half, total_rows) - jnp.maximum(position - half, 0)
        counted = jnp.maximum(counted, 1).astype(f32)
        pooled = (total / counted - both).astype(bf16)
        mixed = jnp.dot(pooled, mix[...], preferred_element_type=f32)
        gated = mixed * (both / (1.0 + jnp.exp(-both)))
        turned[:count] = pltpu.roll(gated, count - REACH, 0)
        branch[...] = turned[...].T[:chans, :rows].astype(bf16)
        turned[:count] = pltpu.roll(acc[:, lanes:], count - REACH, 0)
        ahead[...] = turned[...].T[:, :rows]
        own = acc[ext_rows:, lanes:].astype(bf16)
        for i in range(joint.shape[0]):
            joint[i] = own


def first_layer(mine, other, scaling, gathered, mix, at, chans, ext_rows, total_rows, sp_size):
    chips, count, depth = mine.shape
    lanes = 2 * chans
    rows = ext_rows - 2 * REACH
    padded = -(-count // 128) * 128

    def block(step, at):
        return (step, 0, 0)

    def whole(step, at):
        return (0, 0)

    return pl.pallas_call(
        lambda *refs: first_kernel(chans, rows, ext_rows, total_rows, *refs),
        grid_spec=pltpu.PrefetchScalarGridSpec(
            num_scalar_prefetch=1,
            grid=(chips // PAIR,),
            in_specs=[
                pl.BlockSpec(memory_space=pltpu.VMEM),
                pl.BlockSpec((PAIR, count, depth), block),
                pl.BlockSpec((count, lanes), whole),
                pl.BlockSpec((CORES * PAIR, 2 * lanes, depth), block),
                pl.BlockSpec((lanes, lanes), whole),
            ],
            out_specs=[
                pl.BlockSpec((chans, rows), whole),
                pl.BlockSpec((lanes, rows), whole),
                pl.BlockSpec((sp_size, count - ext_rows, lanes), lambda step, at: (0, 0, 0)),
            ],
            scratch_shapes=[
                pltpu.VMEM((count, 2 * lanes), f32),
                pltpu.VMEM((padded, lanes), f32),
            ],
        ),
        out_shape=[
            jax.ShapeDtypeStruct((chans, rows), bf16),
            jax.ShapeDtypeStruct((lanes, rows), f32),
            jax.ShapeDtypeStruct((sp_size, count - ext_rows, lanes), bf16),
        ],
        compiler_params=pltpu.CompilerParams(dimension_semantics=("arbitrary",), vmem_limit_bytes=28 << 20),
        cost_estimate=pl.CostEstimate(
            flops=CORES * chips * count * depth * 4 * lanes,
            bytes_accessed=CORES * chips * depth * 2 * (count + 2 * lanes),
            transcendentals=0,
        ),
        name="first_layer",
    )(at, mine, other, scaling, gathered, mix)


def mixed_branch(sums, scaling, mix, first_position, total_rows, code):
    rows = sums.shape[1] - 2 * REACH
    chans = sums.shape[0] // 2
    scaled = (sums * scaling[None, :]).astype(bf16).astype(f32)
    pool_in = scaled[chans:]
    gate = window(scaled[:chans], REACH, rows)
    position = first_position + jnp.arange(rows, dtype=jnp.int32)
    half = jnp.left_shift(1, code)
    counted = jnp.minimum(position + half, total_rows) - jnp.maximum(position - half, 0)
    counted = counted.astype(f32)
    running = pool_in
    total = None
    for code_value, size in enumerate((1, 2, 4, 8)):
        width = running.shape[1] - size
        running = window(running, 0, width) + window(running, size, width)
        picked = window(running, REACH - size, rows)
        total = picked if total is None else jnp.where(code == code_value, picked, total)
    pooled = (total / counted[None, :] - window(pool_in, REACH, rows)).astype(bf16)
    mixed = dot0(mix, pooled)
    return (mixed * jax.nn.silu(gate)).astype(bf16)


def local(hidden_in, norm_gain, w_pool_in, w_pool_gate, group_mix, w_out):
    rows, cols = hidden_in.shape
    chans = w_pool_in.shape[2]
    depth = w_pool_in.shape[1]
    out_rows = w_out.shape[1]
    col_rank = lax.axis_index("tp")
    row_rank = lax.axis_index("sp")
    tp_size = lax.axis_size("tp")
    sp_size = lax.axis_size("sp")
    chips = tp_size // CORES
    core = jnp.bitwise_and(col_rank, CORES - 1)
    total_rows = rows * sp_size
    full_width = cols * tp_size
    code = jnp.bitwise_and(col_rank, 3)
    halo = 2 * REACH
    ext_rows = rows + 2 * halo
    lanes = 2 * chans

    packed = packed_weights(w_pool_gate.transpose(0, 2, 1), w_pool_in.transpose(0, 2, 1), w_out, norm_gain, row_rank)
    packed, hidden_in = lax.optimization_barrier((packed, hidden_in))
    gathered = lax.all_gather(packed, "sp", axis=0, tiled=False)

    def last_rows(gathered, layer):
        at = 2 * lanes + layer * out_rows
        return gathered[:, at : at + out_rows].reshape(chips, CORES * out_rows, cols)

    up = [(i, i + 1) for i in range(sp_size - 1)]
    down = [(j, i) for i, j in up]
    before = lax.ppermute(hidden_in[rows - halo :], "sp", up)
    after = lax.ppermute(hidden_in[:halo], "sp", down)
    block = jnp.concatenate([before, hidden_in, after, w_out[0]], axis=0)
    mine = same_core_blocks(block)
    other = swap_cores(mine)

    def by_core(array):
        size = array.shape[1] // CORES
        return [
            lax.dynamic_slice_in_dim(array, c * size, size, axis=1).reshape(-1, array.shape[2]) for c in (core, 1 - core)
        ]

    twins = [[CORES * i + c for i in range(chips)] for c in range(CORES)]

    def over_twins(branch):
        return lax.all_gather(branch, "tp", axis=0, tiled=True, axis_index_groups=twins)

    def product(weights, operands):
        return sum(dot0(weight, operand) for weight, operand in zip(weights, operands))

    mixes = [lax.dynamic_index_in_dim(group_mix[i], col_rank, 0, keepdims=False) for i in range(2)]

    mid_rows = rows + 2 * REACH
    start = row_rank * rows
    mix = jnp.pad(mixes[0], ((chans, 0), (0, chans)))
    scalars = jnp.stack([core, code, start - halo]).astype(jnp.int32)
    scaling = row_scaling(mine, other, full_width)
    branch, ahead, joint = first_layer(
        mine, other, scaling, gathered, mix, scalars, chans, ext_rows, total_rows, sp_size
    )
    joint = exchanged(joint, "sp")
    same = over_twins(branch)
    same, joint, gathered = lax.optimization_barrier((same, joint, gathered))
    joint = joint.reshape(chips, CORES * out_rows, lanes)
    pair = same, swap_cores(same)
    resid = (block[REACH : REACH + mid_rows].T.astype(f32) + product(by_core(last_rows(gathered, 0)), pair)).astype(bf16)
    resid_f = resid.astype(f32)
    square_sum = sent_to_all(jnp.sum(resid_f * resid_f, axis=0), "tp").sum(axis=0)
    scaling = lax.rsqrt(square_sum / full_width + norm_eps)

    sums = ahead + product(by_core(joint), pair)
    branch = mixed_branch(sums, scaling, mixes[1], start, total_rows, code)
    rest = sent_to_all(branch[BLOCKING:], "tp")
    branch = lax.all_gather(branch[:BLOCKING], "tp", axis=0, tiled=True)
    branch, rest = lax.optimization_barrier((branch, rest))
    weight = last_rows(gathered, 1).reshape(tp_size, out_rows, cols)
    resid = window(resid_f, REACH, rows)
    for left, right in ((weight[:, :BLOCKING], branch), (weight[:, BLOCKING:], rest)):
        resid = resid + dot0(left.reshape(-1, cols), right.reshape(-1, rows))
    return resid.astype(bf16).T


def solution(mesh):
    in_specs = (
        P(("grp", "sp"), "tp"),
        P(),
        P(None, "sp", "tp"),
        P(None, "sp", "tp"),
        P(),
        P(None, "sp", "tp"),
    )
    out_specs = P(("grp", "sp"), "tp")
    return jax.shard_map(local, mesh=mesh, in_specs=in_specs, out_specs=out_specs, check_vma=False)
```

```python
import jax
import jax.numpy as jnp
from jax import lax
from jax.experimental import pallas as pl
from jax.experimental.pallas import tpu as pltpu
from jax.sharding import PartitionSpec as P

GROUP = 64
CORES = 2
REACH = 8
PAIR = 4
norm_eps = 1e-06
bf16 = jnp.bfloat16
f32 = jnp.float32


def sent_to_all(array, axis):
    copies = jnp.broadcast_to(array, (lax.axis_size(axis), *array.shape))
    return lax.all_to_all(copies, axis, split_axis=0, concat_axis=0, tiled=True)


def exchanged(copies, axis):
    return lax.all_to_all(copies, axis, split_axis=0, concat_axis=0, tiled=True)


def swap_cores(array):
    size = lax.axis_size("tp")
    return lax.ppermute(array, "tp", [(i, i ^ 1) for i in range(size)])


def shifted_over_chips(array, step):
    size = lax.axis_size("tp")
    return lax.ppermute(array, "tp", [(i, (i + CORES * step) % size) for i in range(size)])


def same_core_blocks(block):
    chips = lax.axis_size("tp") // CORES
    chip = lax.axis_index("tp") // CORES
    out = jnp.zeros((chips, *block.shape), block.dtype)
    origin = (0,) * block.ndim
    out = lax.dynamic_update_slice(out, block[None], (chip, *origin))
    right = left = block
    for step in range(1, chips // 2 + 1):
        right = shifted_over_chips(right, 1)
        out = lax.dynamic_update_slice(out, right[None], ((chip - step) % chips, *origin))
        if step < chips - chips // 2:
            left = shifted_over_chips(left, -1)
            out = lax.dynamic_update_slice(out, left[None], ((chip + step) % chips, *origin))
    return out


def dot0(left, right):
    return lax.dot_general(left, right, (((0,), (0,)), ((), ())), preferred_element_type=f32)


def window(array, start, length):
    return lax.slice_in_dim(array, start, start + length, axis=1)


def pack_kernel(at, w_gate, w_in, w_last, gain, packed):
    layers, chans, _ = w_gate.shape
    rows = 0
    for layer in range(layers):
        for weight in (w_gate, w_in):
            packed[rows : rows + chans] = (weight[layer].astype(f32) * gain[layer : layer + 1]).astype(bf16)
            rows += chans
    for layer in range(layers):
        packed[rows : rows + w_last.shape[1]] = w_last[layer]
        rows += w_last.shape[1]


def packed_weights(w_gate, w_in, w_last, gain, row_rank):
    layers, chans, depth = w_gate.shape
    rows = layers * (2 * chans + w_last.shape[1])

    def whole(array):
        return pl.BlockSpec(array.shape, lambda step, at: (0, 0, 0))

    return pl.pallas_call(
        pack_kernel,
        grid_spec=pltpu.PrefetchScalarGridSpec(
            num_scalar_prefetch=1,
            grid=(1,),
            in_specs=[
                whole(w_gate),
                whole(w_in),
                whole(w_last),
                pl.BlockSpec((layers, depth), lambda step, at: (0, at[0])),
            ],
            out_specs=pl.BlockSpec((rows, depth), lambda step, at: (0, 0)),
        ),
        out_shape=jax.ShapeDtypeStruct((rows, depth), bf16),
        name="packed_weights",
    )(row_rank.reshape(1).astype(jnp.int32), w_gate, w_in, w_last, gain)


def squares_kernel(full_width, mine, other, scaling, squares):
    step = pl.program_id(0)
    lanes = squares.shape[1]

    @pl.when(step == 0)
    def _():
        squares[...] = jnp.zeros_like(squares)

    total = squares[...]
    for block, first in ((mine, PAIR * step), (other, 0)):
        for chip in range(PAIR):
            for i in range(0, block.shape[2], lanes):
                part = block[first + chip, :, i : i + lanes].astype(f32)
                total = total + part * part
    squares[...] = total

    @pl.when(step == pl.num_programs(0) - 1)
    def _():
        mean = jnp.sum(squares[...], axis=1, keepdims=True) / full_width
        scaling[...] = jnp.broadcast_to(lax.rsqrt(mean + norm_eps), scaling.shape)


def row_scaling(mine, other, full_width):
    chips, count, depth = mine.shape
    specs = [pl.BlockSpec(memory_space=pltpu.VMEM), pl.BlockSpec((PAIR, count, depth), lambda step: (step, 0, 0))]
    return pl.pallas_call(
        lambda *refs: squares_kernel(full_width, *refs),
        grid=(chips // PAIR,),
        in_specs=specs,
        out_specs=pl.BlockSpec((count, 128), lambda step: (0, 0)),
        scratch_shapes=[pltpu.VMEM((count, 128), f32)],
        out_shape=jax.ShapeDtypeStruct((count, 128), f32),
        compiler_params=pltpu.CompilerParams(dimension_semantics=("arbitrary",), vmem_limit_bytes=28 << 20),
        cost_estimate=pl.CostEstimate(
            flops=4 * CORES * chips * count * depth, bytes_accessed=CORES * chips * count * depth * 2, transcendentals=0
        ),
        name="row_scaling",
    )(mine, other)


def first_kernel(chans, rows, ext_rows, total_rows, at, mine, other, scaling, w_all, mix, branch, ahead, joint, acc, turned):
    step = pl.program_id(0)
    lanes = 2 * chans
    count = mine.shape[1]
    core = at[0]
    total = 0
    for chip in range(PAIR):
        for part, place in ((mine[PAIR * step + chip], core), (other[chip], 1 - core)):
            weight = w_all[CORES * chip + place]
            total = total + lax.dot_general(
                part, weight, (((1,), (1,)), ((), ())), preferred_element_type=f32
            )

    @pl.when(step == 0)
    def _():
        acc[...] = total

    @pl.when(step > 0)
    def _():
        acc[...] += total

    @pl.when(step == pl.num_programs(0) - 1)
    def _():
        code = at[1]
        both = (acc[:, :lanes] * scaling[...]).astype(bf16).astype(f32)
        running = both
        total = None
        for code_value, size in enumerate((1, 2, 4, 8)):
            running = running + pltpu.roll(running, count - size, 0)
            picked = pltpu.roll(running, size, 0)
            total = picked if total is None else jnp.where(code == code_value, picked, total)
        position = at[2] + lax.broadcasted_iota(jnp.int32, (count, lanes), 0)
        half = jnp.left_shift(1, code)
        counted = jnp.minimum(position + half, total_rows) - jnp.maximum(position - half, 0)
        counted = jnp.maximum(counted, 1).astype(f32)
        pooled = (total / counted - both).astype(bf16)
        mixed = jnp.dot(pooled, mix[...], preferred_element_type=f32)
        gated = mixed * (both / (1.0 + jnp.exp(-both)))
        turned[:count] = pltpu.roll(gated, count - REACH, 0)
        branch[...] = turned[...].T[:chans, :rows].astype(bf16)
        turned[:count] = pltpu.roll(acc[:, lanes:], count - REACH, 0)
        ahead[...] = turned[...].T[:, :rows]
        own = acc[ext_rows:, lanes:].astype(bf16)
        for i in range(joint.shape[0]):
            joint[i] = own


def first_layer(mine, other, scaling, gathered, mix, at, chans, ext_rows, total_rows, sp_size):
    chips, count, depth = mine.shape
    lanes = 2 * chans
    rows = ext_rows - 2 * REACH
    padded = -(-count // 128) * 128

    def block(step, at):
        return (step, 0, 0)

    def whole(step, at):
        return (0, 0)

    return pl.pallas_call(
        lambda *refs: first_kernel(chans, rows, ext_rows, total_rows, *refs),
        grid_spec=pltpu.PrefetchScalarGridSpec(
            num_scalar_prefetch=1,
            grid=(chips // PAIR,),
            in_specs=[
                pl.BlockSpec(memory_space=pltpu.VMEM),
                pl.BlockSpec((PAIR, count, depth), block),
                pl.BlockSpec((count, lanes), whole),
                pl.BlockSpec((CORES * PAIR, 2 * lanes, depth), block),
                pl.BlockSpec((lanes, lanes), whole),
            ],
            out_specs=[
                pl.BlockSpec((chans, rows), whole),
                pl.BlockSpec((lanes, rows), whole),
                pl.BlockSpec((sp_size, count - ext_rows, lanes), lambda step, at: (0, 0, 0)),
            ],
            scratch_shapes=[
                pltpu.VMEM((count, 2 * lanes), f32),
                pltpu.VMEM((padded, lanes), f32),
            ],
        ),
        out_shape=[
            jax.ShapeDtypeStruct((chans, rows), bf16),
            jax.ShapeDtypeStruct((lanes, rows), f32),
            jax.ShapeDtypeStruct((sp_size, count - ext_rows, lanes), bf16),
        ],
        compiler_params=pltpu.CompilerParams(dimension_semantics=("arbitrary",), vmem_limit_bytes=46 << 20),
        cost_estimate=pl.CostEstimate(
            flops=CORES * chips * count * depth * 4 * lanes,
            bytes_accessed=CORES * chips * depth * 2 * (count + 2 * lanes),
            transcendentals=0,
        ),
        name="first_layer",
    )(at, mine, other, scaling, gathered, mix)


def mixed_branch(sums, scaling, mix, first_position, total_rows, code):
    rows = sums.shape[1] - 2 * REACH
    chans = sums.shape[0] // 2
    scaled = (sums * scaling[None, :]).astype(bf16).astype(f32)
    pool_in = scaled[chans:]
    gate = window(scaled[:chans], REACH, rows)
    position = first_position + jnp.arange(rows, dtype=jnp.int32)
    half = jnp.left_shift(1, code)
    counted = jnp.minimum(position + half, total_rows) - jnp.maximum(position - half, 0)
    counted = counted.astype(f32)
    running = pool_in
    total = None
    for code_value, size in enumerate((1, 2, 4, 8)):
        width = running.shape[1] - size
        running = window(running, 0, width) + window(running, size, width)
        picked = window(running, REACH - size, rows)
        total = picked if total is None else jnp.where(code == code_value, picked, total)
    pooled = (total / counted[None, :] - window(pool_in, REACH, rows)).astype(bf16)
    mixed = dot0(mix, pooled)
    return (mixed * jax.nn.silu(gate)).astype(bf16)


def local(hidden_in, norm_gain, w_pool_in, w_pool_gate, group_mix, w_out):
    rows, cols = hidden_in.shape
    chans = w_pool_in.shape[2]
    depth = w_pool_in.shape[1]
    out_rows = w_out.shape[1]
    col_rank = lax.axis_index("tp")
    row_rank = lax.axis_index("sp")
    tp_size = lax.axis_size("tp")
    sp_size = lax.axis_size("sp")
    chips = tp_size // CORES
    core = jnp.bitwise_and(col_rank, CORES - 1)
    total_rows = rows * sp_size
    full_width = cols * tp_size
    code = jnp.bitwise_and(col_rank, 3)
    halo = 2 * REACH
    ext_rows = rows + 2 * halo
    lanes = 2 * chans

    packed = packed_weights(w_pool_gate.transpose(0, 2, 1), w_pool_in.transpose(0, 2, 1), w_out, norm_gain, row_rank)
    packed, hidden_in = lax.optimization_barrier((packed, hidden_in))
    gathered = lax.all_gather(packed, "sp", axis=0, tiled=False)

    def last_rows(gathered, layer):
        at = 2 * lanes + layer * out_rows
        return gathered[:, at : at + out_rows].reshape(chips, CORES * out_rows, cols)

    up = [(i, i + 1) for i in range(sp_size - 1)]
    down = [(j, i) for i, j in up]
    before = lax.ppermute(hidden_in[rows - halo :], "sp", up)
    after = lax.ppermute(hidden_in[:halo], "sp", down)
    block = jnp.concatenate([before, hidden_in, after, w_out[0]], axis=0)
    mine = same_core_blocks(block)
    other = swap_cores(mine)

    def by_core(array):
        size = array.shape[1] // CORES
        return [
            lax.dynamic_slice_in_dim(array, c * size, size, axis=1).reshape(-1, array.shape[2]) for c in (core, 1 - core)
        ]

    twins = [[CORES * i + c for i in range(chips)] for c in range(CORES)]

    def over_twins(branch):
        return lax.all_gather(branch, "tp", axis=0, tiled=True, axis_index_groups=twins)

    def product(weights, operands):
        return sum(dot0(weight, operand) for weight, operand in zip(weights, operands))

    mixes = [lax.dynamic_index_in_dim(group_mix[i], col_rank, 0, keepdims=False) for i in range(2)]

    mid_rows = rows + 2 * REACH
    start = row_rank * rows
    mix = jnp.pad(mixes[0], ((chans, 0), (0, chans)))
    scalars = jnp.stack([core, code, start - halo]).astype(jnp.int32)
    scaling = row_scaling(mine, other, full_width)
    branch, ahead, joint = first_layer(
        mine, other, scaling, gathered, mix, scalars, chans, ext_rows, total_rows, sp_size
    )
    joint = exchanged(joint, "sp")
    same = over_twins(branch)
    same, joint, gathered = lax.optimization_barrier((same, joint, gathered))
    joint = joint.reshape(chips, CORES * out_rows, lanes)
    pair = same, swap_cores(same)
    delta = product(pair, by_core(last_rows(gathered, 0)))
    resid = (block[REACH : REACH + mid_rows].astype(f32) + delta).astype(bf16)
    resid_f = resid.astype(f32)
    square_sum = sent_to_all(jnp.sum(resid_f * resid_f, axis=1), "tp").sum(axis=0)
    scaling = lax.rsqrt(square_sum / full_width + norm_eps)

    sums = ahead + product(by_core(joint), pair)
    branch = mixed_branch(sums, scaling, mixes[1], start, total_rows, code)
    same = over_twins(branch)
    pair = same, swap_cores(same)
    resid = resid_f[REACH : REACH + rows] + product(pair, by_core(last_rows(gathered, 1)))
    return resid.astype(bf16)


def solution(mesh):
    in_specs = (
        P(("grp", "sp"), "tp"),
        P(),
        P(None, "sp", "tp"),
        P(None, "sp", "tp"),
        P(),
        P(None, "sp", "tp"),
    )
    out_specs = P(("grp", "sp"), "tp")
    return jax.shard_map(local, mesh=mesh, in_specs=in_specs, out_specs=out_specs, check_vma=False)
```

```python
import jax
import jax.numpy as jnp
from jax import lax
from jax.experimental import pallas as pl
from jax.experimental.pallas import tpu as pltpu
from jax.sharding import PartitionSpec as P

GROUP = 64
CORES = 2
REACH = 8
PAIR = 4
norm_eps = 1e-06
bf16 = jnp.bfloat16
f32 = jnp.float32


def sent_to_all(array, axis):
    copies = jnp.broadcast_to(array, (lax.axis_size(axis), *array.shape))
    return lax.all_to_all(copies, axis, split_axis=0, concat_axis=0, tiled=True)


def exchanged(copies, axis):
    return lax.all_to_all(copies, axis, split_axis=0, concat_axis=0, tiled=True)


def swap_cores(array):
    size = lax.axis_size("tp")
    return lax.ppermute(array, "tp", [(i, i ^ 1) for i in range(size)])


def shifted_over_chips(array, step):
    size = lax.axis_size("tp")
    return lax.ppermute(array, "tp", [(i, (i + CORES * step) % size) for i in range(size)])


def same_core_blocks(block):
    chips = lax.axis_size("tp") // CORES
    chip = lax.axis_index("tp") // CORES
    out = jnp.zeros((chips, *block.shape), block.dtype)
    origin = (0,) * block.ndim
    out = lax.dynamic_update_slice(out, block[None], (chip, *origin))
    right = left = block
    for step in range(1, chips // 2 + 1):
        right = shifted_over_chips(right, 1)
        out = lax.dynamic_update_slice(out, right[None], ((chip - step) % chips, *origin))
        if step < chips - chips // 2:
            left = shifted_over_chips(left, -1)
            out = lax.dynamic_update_slice(out, left[None], ((chip + step) % chips, *origin))
    return out


def dot0(left, right):
    return lax.dot_general(left, right, (((0,), (0,)), ((), ())), preferred_element_type=f32)


def window(array, start, length):
    return lax.slice_in_dim(array, start, start + length, axis=1)


def pack_kernel(at, w_gate, w_in, w_last, gain, packed):
    layers, chans, _ = w_gate.shape
    rows = 0
    for layer in range(layers):
        for weight in (w_gate, w_in):
            packed[rows : rows + chans] = (weight[layer].astype(f32) * gain[layer : layer + 1]).astype(bf16)
            rows += chans
    for layer in range(layers):
        packed[rows : rows + w_last.shape[1]] = w_last[layer]
        rows += w_last.shape[1]


def packed_weights(w_gate, w_in, w_last, gain, row_rank):
    layers, chans, depth = w_gate.shape
    rows = layers * (2 * chans + w_last.shape[1])

    def whole(array):
        return pl.BlockSpec(array.shape, lambda step, at: (0, 0, 0))

    return pl.pallas_call(
        pack_kernel,
        grid_spec=pltpu.PrefetchScalarGridSpec(
            num_scalar_prefetch=1,
            grid=(1,),
            in_specs=[
                whole(w_gate),
                whole(w_in),
                whole(w_last),
                pl.BlockSpec((layers, depth), lambda step, at: (0, at[0])),
            ],
            out_specs=pl.BlockSpec((rows, depth), lambda step, at: (0, 0)),
        ),
        out_shape=jax.ShapeDtypeStruct((rows, depth), bf16),
        name="packed_weights",
    )(row_rank.reshape(1).astype(jnp.int32), w_gate, w_in, w_last, gain)


def squares_kernel(full_width, mine, other, scaling, squares):
    step = pl.program_id(0)
    lanes = squares.shape[1]

    @pl.when(step == 0)
    def _():
        squares[...] = jnp.zeros_like(squares)

    total = squares[...]
    for block, first in ((mine, PAIR * step), (other, 0)):
        for chip in range(PAIR):
            for i in range(0, block.shape[2], lanes):
                part = block[first + chip, :, i : i + lanes].astype(f32)
                total = total + part * part
    squares[...] = total

    @pl.when(step == pl.num_programs(0) - 1)
    def _():
        mean = jnp.sum(squares[...], axis=1, keepdims=True) / full_width
        scaling[...] = jnp.broadcast_to(lax.rsqrt(mean + norm_eps), scaling.shape)


def row_scaling(mine, other, full_width):
    chips, count, depth = mine.shape
    specs = [pl.BlockSpec(memory_space=pltpu.VMEM), pl.BlockSpec((PAIR, count, depth), lambda step: (step, 0, 0))]
    return pl.pallas_call(
        lambda *refs: squares_kernel(full_width, *refs),
        grid=(chips // PAIR,),
        in_specs=specs,
        out_specs=pl.BlockSpec((count, 128), lambda step: (0, 0)),
        scratch_shapes=[pltpu.VMEM((count, 128), f32)],
        out_shape=jax.ShapeDtypeStruct((count, 128), f32),
        compiler_params=pltpu.CompilerParams(dimension_semantics=("arbitrary",), vmem_limit_bytes=28 << 20),
        cost_estimate=pl.CostEstimate(
            flops=4 * CORES * chips * count * depth, bytes_accessed=CORES * chips * count * depth * 2, transcendentals=0
        ),
        name="row_scaling",
    )(mine, other)


def first_kernel(chans, rows, ext_rows, total_rows, at, mine, other, scaling, w_all, mix, branch, ahead, joint, acc, turned):
    step = pl.program_id(0)
    lanes = 2 * chans
    count = mine.shape[1]
    core = at[0]
    total = 0
    for chip in range(PAIR):
        for part, place in ((mine[PAIR * step + chip], core), (other[chip], 1 - core)):
            weight = w_all[CORES * chip + place]
            total = total + lax.dot_general(
                part, weight, (((1,), (1,)), ((), ())), preferred_element_type=f32
            )

    @pl.when(step == 0)
    def _():
        acc[...] = total

    @pl.when(step > 0)
    def _():
        acc[...] += total

    @pl.when(step == pl.num_programs(0) - 1)
    def _():
        code = at[1]
        both = (acc[:, :lanes] * scaling[...]).astype(bf16).astype(f32)
        running = both
        total = None
        for code_value, size in enumerate((1, 2, 4, 8)):
            running = running + pltpu.roll(running, count - size, 0)
            picked = pltpu.roll(running, size, 0)
            total = picked if total is None else jnp.where(code == code_value, picked, total)
        position = at[2] + lax.broadcasted_iota(jnp.int32, (count, lanes), 0)
        half = jnp.left_shift(1, code)
        counted = jnp.minimum(position + half, total_rows) - jnp.maximum(position - half, 0)
        counted = jnp.maximum(counted, 1).astype(f32)
        pooled = (total / counted - both).astype(bf16)
        mixed = jnp.dot(pooled, mix[...], preferred_element_type=f32)
        gated = mixed * (both / (1.0 + jnp.exp(-both)))
        turned[:count] = pltpu.roll(gated, count - REACH, 0)
        branch[...] = turned[...].T[:chans, :rows].astype(bf16)
        turned[:count] = pltpu.roll(acc[:, lanes:], count - REACH, 0)
        ahead[...] = turned[...].T[:, :rows]
        own = acc[ext_rows:, lanes:].astype(bf16)
        for i in range(joint.shape[0]):
            joint[i] = own


def first_layer(mine, other, scaling, gathered, mix, at, chans, ext_rows, total_rows, sp_size):
    chips, count, depth = mine.shape
    lanes = 2 * chans
    rows = ext_rows - 2 * REACH
    padded = -(-count // 128) * 128

    def block(step, at):
        return (step, 0, 0)

    def whole(step, at):
        return (0, 0)

    return pl.pallas_call(
        lambda *refs: first_kernel(chans, rows, ext_rows, total_rows, *refs),
        grid_spec=pltpu.PrefetchScalarGridSpec(
            num_scalar_prefetch=1,
            grid=(chips // PAIR,),
            in_specs=[
                pl.BlockSpec(memory_space=pltpu.VMEM),
                pl.BlockSpec((PAIR, count, depth), block),
                pl.BlockSpec((count, lanes), whole),
                pl.BlockSpec((CORES * PAIR, 2 * lanes, depth), block),
                pl.BlockSpec((lanes, lanes), whole),
            ],
            out_specs=[
                pl.BlockSpec((chans, rows), whole),
                pl.BlockSpec((lanes, rows), whole),
                pl.BlockSpec((sp_size, count - ext_rows, lanes), lambda step, at: (0, 0, 0)),
            ],
            scratch_shapes=[
                pltpu.VMEM((count, 2 * lanes), f32),
                pltpu.VMEM((padded, lanes), f32),
            ],
        ),
        out_shape=[
            jax.ShapeDtypeStruct((chans, rows), bf16),
            jax.ShapeDtypeStruct((lanes, rows), f32),
            jax.ShapeDtypeStruct((sp_size, count - ext_rows, lanes), bf16),
        ],
        compiler_params=pltpu.CompilerParams(dimension_semantics=("arbitrary",), vmem_limit_bytes=46 << 20),
        cost_estimate=pl.CostEstimate(
            flops=CORES * chips * count * depth * 4 * lanes,
            bytes_accessed=CORES * chips * depth * 2 * (count + 2 * lanes),
            transcendentals=0,
        ),
        name="first_layer",
    )(at, mine, other, scaling, gathered, mix)


def mixed_branch(sums, scaling, mix, first_position, total_rows, code):
    rows = sums.shape[1] - 2 * REACH
    chans = sums.shape[0] // 2
    scaled = (sums * scaling[None, :]).astype(bf16).astype(f32)
    pool_in = scaled[chans:]
    gate = window(scaled[:chans], REACH, rows)
    position = first_position + jnp.arange(rows, dtype=jnp.int32)
    half = jnp.left_shift(1, code)
    counted = jnp.minimum(position + half, total_rows) - jnp.maximum(position - half, 0)
    counted = counted.astype(f32)
    running = pool_in
    total = None
    for code_value, size in enumerate((1, 2, 4, 8)):
        width = running.shape[1] - size
        running = window(running, 0, width) + window(running, size, width)
        picked = window(running, REACH - size, rows)
        total = picked if total is None else jnp.where(code == code_value, picked, total)
    pooled = (total / counted[None, :] - window(pool_in, REACH, rows)).astype(bf16)
    mixed = dot0(mix, pooled)
    return (mixed * jax.nn.silu(gate)).astype(bf16)


def local(hidden_in, norm_gain, w_pool_in, w_pool_gate, group_mix, w_out):
    rows, cols = hidden_in.shape
    chans = w_pool_in.shape[2]
    depth = w_pool_in.shape[1]
    out_rows = w_out.shape[1]
    col_rank = lax.axis_index("tp")
    row_rank = lax.axis_index("sp")
    tp_size = lax.axis_size("tp")
    sp_size = lax.axis_size("sp")
    chips = tp_size // CORES
    core = jnp.bitwise_and(col_rank, CORES - 1)
    total_rows = rows * sp_size
    full_width = cols * tp_size
    code = jnp.bitwise_and(col_rank, 3)
    halo = 2 * REACH
    ext_rows = rows + 2 * halo
    lanes = 2 * chans

    packed = packed_weights(w_pool_gate.transpose(0, 2, 1), w_pool_in.transpose(0, 2, 1), w_out, norm_gain, row_rank)
    packed, hidden_in = lax.optimization_barrier((packed, hidden_in))
    gathered = lax.all_gather(packed, "sp", axis=0, tiled=False)

    def last_rows(gathered, layer):
        at = 2 * lanes + layer * out_rows
        return gathered[:, at : at + out_rows].reshape(chips, CORES * out_rows, cols)

    up = [(i, i + 1) for i in range(sp_size - 1)]
    down = [(j, i) for i, j in up]
    before = lax.ppermute(hidden_in[rows - halo :], "sp", up)
    after = lax.ppermute(hidden_in[:halo], "sp", down)
    block = jnp.concatenate([before, hidden_in, after, w_out[0]], axis=0)
    mine = same_core_blocks(block)
    other = swap_cores(mine)

    chip = col_rank // CORES
    ring = jnp.bitwise_and(chip + core, 1)

    def by_ring(array):
        size = array.shape[1] // CORES
        paired = array.reshape(chips // 2, 2 * CORES, size, array.shape[2])
        sides = []
        for c in (ring, 1 - ring):
            picked = [lax.dynamic_slice_in_dim(paired, at, 1, axis=1) for at in (c, CORES + 1 - c)]
            sides.append(jnp.concatenate(picked, axis=1).reshape(-1, array.shape[2]))
        return sides

    twins = [[CORES * i + (i + c) % CORES for i in range(chips)] for c in range(CORES)]

    def over_twins(branch):
        return lax.all_gather(branch, "tp", axis=0, tiled=True, axis_index_groups=twins)

    def product(weights, operands):
        return sum(dot0(weight, operand) for weight, operand in zip(weights, operands))

    mixes = [lax.dynamic_index_in_dim(group_mix[i], col_rank, 0, keepdims=False) for i in range(2)]

    mid_rows = rows + 2 * REACH
    start = row_rank * rows
    mix = jnp.pad(mixes[0], ((chans, 0), (0, chans)))
    scalars = jnp.stack([core, code, start - halo]).astype(jnp.int32)
    scaling = row_scaling(mine, other, full_width)
    branch, ahead, joint = first_layer(
        mine, other, scaling, gathered, mix, scalars, chans, ext_rows, total_rows, sp_size
    )
    joint = exchanged(joint, "sp")
    same = over_twins(branch)
    same, joint, gathered = lax.optimization_barrier((same, joint, gathered))
    joint = joint.reshape(chips, CORES * out_rows, lanes)
    pair = same, swap_cores(same)
    delta = product(pair, by_ring(last_rows(gathered, 0)))
    resid = (block[REACH : REACH + mid_rows].astype(f32) + delta).astype(bf16)
    resid_f = resid.astype(f32)
    square_sum = sent_to_all(jnp.sum(resid_f * resid_f, axis=1), "tp").sum(axis=0)
    scaling = lax.rsqrt(square_sum / full_width + norm_eps)

    sums = ahead + product(by_ring(joint), pair)
    branch = mixed_branch(sums, scaling, mixes[1], start, total_rows, code)
    same = over_twins(branch)
    pair = same, swap_cores(same)
    resid = resid_f[REACH : REACH + rows] + product(pair, by_ring(last_rows(gathered, 1)))
    return resid.astype(bf16)


def solution(mesh):
    in_specs = (
        P(("grp", "sp"), "tp"),
        P(),
        P(None, "sp", "tp"),
        P(None, "sp", "tp"),
        P(),
        P(None, "sp", "tp"),
    )
    out_specs = P(("grp", "sp"), "tp")
    return jax.shard_map(local, mesh=mesh, in_specs=in_specs, out_specs=out_specs, check_vma=False)
```

```python
import jax
import jax.numpy as jnp
from jax import lax
from jax.experimental import pallas as pl
from jax.experimental.pallas import tpu as pltpu
from jax.sharding import PartitionSpec as P

CORES = 2
REACH = 8
PAIR = 4
norm_eps = 1e-06
bf16 = jnp.bfloat16
f32 = jnp.float32


def sent_to_all(array, axis):
    copies = jnp.broadcast_to(array, (lax.axis_size(axis), *array.shape))
    return lax.all_to_all(copies, axis, split_axis=0, concat_axis=0, tiled=True)


def exchanged(copies, axis):
    return lax.all_to_all(copies, axis, split_axis=0, concat_axis=0, tiled=True)


def swap_cores(array):
    size = lax.axis_size("tp")
    return lax.ppermute(array, "tp", [(i, i ^ 1) for i in range(size)])


def shifted_over_chips(array, step):
    size = lax.axis_size("tp")
    return lax.ppermute(array, "tp", [(i, (i + CORES * step) % size) for i in range(size)])


def same_core_blocks(block):
    chips = lax.axis_size("tp") // CORES
    chip = lax.axis_index("tp") // CORES
    out = jnp.zeros((chips, *block.shape), block.dtype)
    origin = (0,) * block.ndim
    out = lax.dynamic_update_slice(out, block[None], (chip, *origin))
    right = left = block
    for step in range(1, chips // 2 + 1):
        right = shifted_over_chips(right, 1)
        out = lax.dynamic_update_slice(out, right[None], ((chip - step) % chips, *origin))
        if step < chips - chips // 2:
            left = shifted_over_chips(left, -1)
            out = lax.dynamic_update_slice(out, left[None], ((chip + step) % chips, *origin))
    return out


def dot0(left, right):
    return lax.dot_general(left, right, (((0,), (0,)), ((), ())), preferred_element_type=f32)


def window(array, start, length):
    return lax.slice_in_dim(array, start, start + length, axis=1)


def pack_kernel(at, w_gate, w_in, w_last, gain, packed):
    layers, chans, _ = w_gate.shape
    rows = 0
    for layer in range(layers):
        for weight in (w_gate, w_in):
            packed[rows : rows + chans] = (weight[layer].astype(f32) * gain[layer : layer + 1]).astype(bf16)
            rows += chans
    for layer in range(layers):
        packed[rows : rows + w_last.shape[1]] = w_last[layer]
        rows += w_last.shape[1]


def packed_weights(w_gate, w_in, w_last, gain, row_rank):
    layers, chans, depth = w_gate.shape
    rows = layers * (2 * chans + w_last.shape[1])

    def whole(array):
        return pl.BlockSpec(array.shape, lambda step, at: (0, 0, 0))

    return pl.pallas_call(
        pack_kernel,
        grid_spec=pltpu.PrefetchScalarGridSpec(
            num_scalar_prefetch=1,
            grid=(1,),
            in_specs=[
                whole(w_gate),
                whole(w_in),
                whole(w_last),
                pl.BlockSpec((layers, depth), lambda step, at: (0, at[0])),
            ],
            out_specs=pl.BlockSpec((rows, depth), lambda step, at: (0, 0)),
        ),
        out_shape=jax.ShapeDtypeStruct((rows, depth), bf16),
        name="packed_weights",
    )(row_rank.reshape(1).astype(jnp.int32), w_gate, w_in, w_last, gain)


def squares_kernel(full_width, mine, other, scaling, squares):
    step = pl.program_id(0)
    lanes = squares.shape[1]

    @pl.when(step == 0)
    def _():
        squares[...] = jnp.zeros_like(squares)

    total = squares[...]
    for block, first in ((mine, PAIR * step), (other, 0)):
        for chip in range(PAIR):
            for i in range(0, block.shape[2], lanes):
                part = block[first + chip, :, i : i + lanes].astype(f32)
                total = total + part * part
    squares[...] = total

    @pl.when(step == pl.num_programs(0) - 1)
    def _():
        mean = jnp.sum(squares[...], axis=1, keepdims=True) / full_width
        scaling[...] = jnp.broadcast_to(lax.rsqrt(mean + norm_eps), scaling.shape)


def row_scaling(mine, other, full_width):
    chips, count, depth = mine.shape
    specs = [pl.BlockSpec(memory_space=pltpu.VMEM), pl.BlockSpec((PAIR, count, depth), lambda step: (step, 0, 0))]
    return pl.pallas_call(
        lambda *refs: squares_kernel(full_width, *refs),
        grid=(chips // PAIR,),
        in_specs=specs,
        out_specs=pl.BlockSpec((count, 128), lambda step: (0, 0)),
        scratch_shapes=[pltpu.VMEM((count, 128), f32)],
        out_shape=jax.ShapeDtypeStruct((count, 128), f32),
        compiler_params=pltpu.CompilerParams(dimension_semantics=("arbitrary",), vmem_limit_bytes=28 << 20),
        cost_estimate=pl.CostEstimate(
            flops=4 * CORES * chips * count * depth, bytes_accessed=CORES * chips * count * depth * 2, transcendentals=0
        ),
        name="row_scaling",
    )(mine, other)


def first_kernel(chans, rows, ext_rows, total_rows, at, mine, other, scaling, w_all, mix, branch, ahead, joint, acc, turned):
    step = pl.program_id(0)
    lanes = 2 * chans
    count = mine.shape[1]
    core = at[0]
    total = 0
    for chip in range(PAIR):
        for part, place in ((mine[PAIR * step + chip], core), (other[chip], 1 - core)):
            weight = w_all[CORES * chip + place]
            total = total + lax.dot_general(
                part, weight, (((1,), (1,)), ((), ())), preferred_element_type=f32
            )

    @pl.when(step == 0)
    def _():
        acc[...] = total

    @pl.when(step > 0)
    def _():
        acc[...] += total

    @pl.when(step == pl.num_programs(0) - 1)
    def _():
        code = at[1]
        both = (acc[:, :lanes] * scaling[...]).astype(bf16).astype(f32)
        running = both
        total = None
        for code_value, size in enumerate((1, 2, 4, 8)):
            running = running + pltpu.roll(running, count - size, 0)
            picked = pltpu.roll(running, size, 0)
            total = picked if total is None else jnp.where(code == code_value, picked, total)
        position = at[2] + lax.broadcasted_iota(jnp.int32, (count, lanes), 0)
        half = jnp.left_shift(1, code)
        counted = jnp.minimum(position + half, total_rows) - jnp.maximum(position - half, 0)
        counted = jnp.maximum(counted, 1).astype(f32)
        pooled = (total / counted - both).astype(bf16)
        mixed = jnp.dot(pooled, mix[...], preferred_element_type=f32)
        gated = mixed * (both / (1.0 + jnp.exp(-both)))
        turned[:count] = pltpu.roll(gated, count - REACH, 0)
        branch[...] = turned[...].T[:chans, :rows].astype(bf16)
        turned[:count] = pltpu.roll(acc[:, lanes:], count - REACH, 0)
        ahead[...] = turned[...].T[:, :rows]
        own = acc[ext_rows:, lanes:].astype(bf16)
        for i in range(joint.shape[0]):
            joint[i] = own


def first_layer(mine, other, scaling, gathered, mix, at, chans, ext_rows, total_rows, sp_size):
    chips, count, depth = mine.shape
    lanes = 2 * chans
    rows = ext_rows - 2 * REACH
    padded = -(-count // 128) * 128

    def block(step, at):
        return (step, 0, 0)

    def whole(step, at):
        return (0, 0)

    return pl.pallas_call(
        lambda *refs: first_kernel(chans, rows, ext_rows, total_rows, *refs),
        grid_spec=pltpu.PrefetchScalarGridSpec(
            num_scalar_prefetch=1,
            grid=(chips // PAIR,),
            in_specs=[
                pl.BlockSpec(memory_space=pltpu.VMEM),
                pl.BlockSpec((PAIR, count, depth), block),
                pl.BlockSpec((count, lanes), whole),
                pl.BlockSpec((CORES * PAIR, 2 * lanes, depth), block),
                pl.BlockSpec((lanes, lanes), whole),
            ],
            out_specs=[
                pl.BlockSpec((chans, rows), whole),
                pl.BlockSpec((lanes, rows), whole),
                pl.BlockSpec((sp_size, count - ext_rows, lanes), lambda step, at: (0, 0, 0)),
            ],
            scratch_shapes=[
                pltpu.VMEM((count, 2 * lanes), f32),
                pltpu.VMEM((padded, lanes), f32),
            ],
        ),
        out_shape=[
            jax.ShapeDtypeStruct((chans, rows), bf16),
            jax.ShapeDtypeStruct((lanes, rows), f32),
            jax.ShapeDtypeStruct((sp_size, count - ext_rows, lanes), bf16),
        ],
        compiler_params=pltpu.CompilerParams(dimension_semantics=("arbitrary",), vmem_limit_bytes=46 << 20),
        cost_estimate=pl.CostEstimate(
            flops=CORES * chips * count * depth * 4 * lanes,
            bytes_accessed=CORES * chips * depth * 2 * (count + 2 * lanes),
            transcendentals=0,
        ),
        name="first_layer",
    )(at, mine, other, scaling, gathered, mix)


def mixed_branch(sums, scaling, mix, first_position, total_rows, code):
    rows = sums.shape[1] - 2 * REACH
    chans = sums.shape[0] // 2
    scaled = (sums * scaling[None, :]).astype(bf16).astype(f32)
    pool_in = scaled[chans:]
    gate = window(scaled[:chans], REACH, rows)
    position = first_position + jnp.arange(rows, dtype=jnp.int32)
    half = jnp.left_shift(1, code)
    counted = jnp.minimum(position + half, total_rows) - jnp.maximum(position - half, 0)
    counted = counted.astype(f32)
    running = pool_in
    total = None
    for code_value, size in enumerate((1, 2, 4, 8)):
        width = running.shape[1] - size
        running = window(running, 0, width) + window(running, size, width)
        picked = window(running, REACH - size, rows)
        total = picked if total is None else jnp.where(code == code_value, picked, total)
    pooled = (total / counted[None, :] - window(pool_in, REACH, rows)).astype(bf16)
    mixed = dot0(mix, pooled)
    return (mixed * jax.nn.silu(gate)).astype(bf16)


def local(hidden_in, norm_gain, w_pool_in, w_pool_gate, group_mix, w_out):
    rows, cols = hidden_in.shape
    chans = w_pool_in.shape[2]
    out_rows = w_out.shape[1]
    col_rank = lax.axis_index("tp")
    row_rank = lax.axis_index("sp")
    tp_size = lax.axis_size("tp")
    sp_size = lax.axis_size("sp")
    chips = tp_size // CORES
    core = jnp.bitwise_and(col_rank, CORES - 1)
    total_rows = rows * sp_size
    full_width = cols * tp_size
    code = jnp.bitwise_and(col_rank, 3)
    halo = 2 * REACH
    ext_rows = rows + 2 * halo
    lanes = 2 * chans

    packed = packed_weights(w_pool_gate.transpose(0, 2, 1), w_pool_in.transpose(0, 2, 1), w_out, norm_gain, row_rank)
    packed, hidden_in = lax.optimization_barrier((packed, hidden_in))
    gathered = lax.all_gather(packed, "sp", axis=0, tiled=False)

    def last_rows(gathered, layer):
        at = 2 * lanes + layer * out_rows
        return gathered[:, at : at + out_rows].reshape(chips, CORES * out_rows, cols)

    up = [(i, i + 1) for i in range(sp_size - 1)]
    down = [(j, i) for i, j in up]
    before = lax.ppermute(hidden_in[rows - halo :], "sp", up)
    after = lax.ppermute(hidden_in[:halo], "sp", down)
    block = jnp.concatenate([before, hidden_in, after, w_out[0]], axis=0)
    mine = same_core_blocks(block)
    other = swap_cores(mine)

    chip = col_rank // CORES
    ring = jnp.bitwise_and(chip + core, 1)

    def by_ring(array):
        size = array.shape[1] // CORES
        paired = array.reshape(chips // 2, 2 * CORES, size, array.shape[2])
        sides = []
        for c in (ring, 1 - ring):
            picked = [lax.dynamic_slice_in_dim(paired, at, 1, axis=1) for at in (c, CORES + 1 - c)]
            sides.append(jnp.concatenate(picked, axis=1).reshape(-1, array.shape[2]))
        return sides

    twins = [[CORES * i + (i + c) % CORES for i in range(chips)] for c in range(CORES)]

    def over_twins(branch):
        return lax.all_gather(branch, "tp", axis=0, tiled=True, axis_index_groups=twins)

    def product(weights, operands):
        return sum(dot0(weight, operand) for weight, operand in zip(weights, operands))

    mixes = [lax.dynamic_index_in_dim(group_mix[i], col_rank, 0, keepdims=False) for i in range(2)]

    mid_rows = rows + 2 * REACH
    start = row_rank * rows
    mix = jnp.pad(mixes[0], ((chans, 0), (0, chans)))
    scalars = jnp.stack([core, code, start - halo]).astype(jnp.int32)
    scaling = row_scaling(mine, other, full_width)
    branch, ahead, joint = first_layer(
        mine, other, scaling, gathered, mix, scalars, chans, ext_rows, total_rows, sp_size
    )
    joint = exchanged(joint, "sp")
    same = over_twins(branch)
    same, joint, gathered = lax.optimization_barrier((same, joint, gathered))
    joint = joint.reshape(chips, CORES * out_rows, lanes)
    other = swap_cores(same)
    pair = same, other
    delta = product(pair, by_ring(last_rows(gathered, 0)))
    resid = (block[REACH : REACH + mid_rows].astype(f32) + delta).astype(bf16)
    resid_f = resid.astype(f32)
    square_sum = sent_to_all(jnp.sum(resid_f * resid_f, axis=1), "tp").sum(axis=0)
    scaling = lax.rsqrt(square_sum / full_width + norm_eps)

    sums = ahead + product(by_ring(joint), pair)
    branch = mixed_branch(sums, scaling, mixes[1], start, total_rows, code)
    same = over_twins(branch)
    pair = same, swap_cores(same)
    resid = resid_f[REACH : REACH + rows] + product(pair, by_ring(last_rows(gathered, 1)))
    return resid.astype(bf16)


def solution(mesh):
    in_specs = (
        P(("grp", "sp"), "tp"),
        P(),
        P(None, "sp", "tp"),
        P(None, "sp", "tp"),
        P(),
        P(None, "sp", "tp"),
    )
    out_specs = P(("grp", "sp"), "tp")
    return jax.shard_map(local, mesh=mesh, in_specs=in_specs, out_specs=out_specs, check_vma=False)
```

```python
import jax
import jax.numpy as jnp
from jax import lax
from jax.experimental import pallas as pl
from jax.experimental.pallas import tpu as pltpu
from jax.sharding import PartitionSpec as P

CORES = 2
REACH = 8
PAIR = 4
norm_eps = 1e-06
bf16 = jnp.bfloat16
f32 = jnp.float32


def sent_to_all(array, axis):
    copies = jnp.broadcast_to(array, (lax.axis_size(axis), *array.shape))
    return lax.all_to_all(copies, axis, split_axis=0, concat_axis=0, tiled=True)


def exchanged(copies, axis):
    return lax.all_to_all(copies, axis, split_axis=0, concat_axis=0, tiled=True)


def swap_cores(array):
    size = lax.axis_size("tp")
    return lax.ppermute(array, "tp", [(i, i ^ 1) for i in range(size)])


def shifted_over_chips(array, step):
    size = lax.axis_size("tp")
    return lax.ppermute(array, "tp", [(i, (i + CORES * step) % size) for i in range(size)])


def same_core_blocks(block):
    chips = lax.axis_size("tp") // CORES
    chip = lax.axis_index("tp") // CORES
    out = jnp.zeros((chips, *block.shape), block.dtype)
    origin = (0,) * block.ndim
    out = lax.dynamic_update_slice(out, block[None], (chip, *origin))
    right = left = block
    for step in range(1, chips // 2 + 1):
        right = shifted_over_chips(right, 1)
        out = lax.dynamic_update_slice(out, right[None], ((chip - step) % chips, *origin))
        if step < chips - chips // 2:
            left = shifted_over_chips(left, -1)
            out = lax.dynamic_update_slice(out, left[None], ((chip + step) % chips, *origin))
    return out


def dot0(left, right):
    return lax.dot_general(left, right, (((0,), (0,)), ((), ())), preferred_element_type=f32)


def window(array, start, length):
    return lax.slice_in_dim(array, start, start + length, axis=1)


def pack_kernel(at, w_gate, w_in, w_last, gain, packed):
    layers, chans, _ = w_gate.shape
    rows = 0
    for layer in range(layers):
        for weight in (w_gate, w_in):
            packed[rows : rows + chans] = (weight[layer].astype(f32) * gain[layer : layer + 1]).astype(bf16)
            rows += chans
    for layer in range(layers):
        packed[rows : rows + w_last.shape[1]] = w_last[layer]
        rows += w_last.shape[1]


def packed_weights(w_gate, w_in, w_last, gain, row_rank):
    layers, chans, depth = w_gate.shape
    rows = layers * (2 * chans + w_last.shape[1])

    def whole(array):
        return pl.BlockSpec(array.shape, lambda step, at: (0, 0, 0))

    return pl.pallas_call(
        pack_kernel,
        grid_spec=pltpu.PrefetchScalarGridSpec(
            num_scalar_prefetch=1,
            grid=(1,),
            in_specs=[
                whole(w_gate),
                whole(w_in),
                whole(w_last),
                pl.BlockSpec((layers, depth), lambda step, at: (0, at[0])),
            ],
            out_specs=pl.BlockSpec((rows, depth), lambda step, at: (0, 0)),
        ),
        out_shape=jax.ShapeDtypeStruct((rows, depth), bf16),
        name="packed_weights",
    )(row_rank.reshape(1).astype(jnp.int32), w_gate, w_in, w_last, gain)


def squares_kernel(full_width, mine, other, scaling, squares):
    step = pl.program_id(0)
    lanes = squares.shape[1]

    @pl.when(step == 0)
    def _():
        squares[...] = jnp.zeros_like(squares)

    total = squares[...]
    for block, first in ((mine, PAIR * step), (other, 0)):
        for chip in range(PAIR):
            for i in range(0, block.shape[2], lanes):
                part = block[first + chip, :, i : i + lanes].astype(f32)
                total = total + part * part
    squares[...] = total

    @pl.when(step == pl.num_programs(0) - 1)
    def _():
        mean = jnp.sum(squares[...], axis=1, keepdims=True) / full_width
        scaling[...] = jnp.broadcast_to(lax.rsqrt(mean + norm_eps), scaling.shape)


def row_scaling(mine, other, full_width):
    chips, count, depth = mine.shape
    specs = [pl.BlockSpec(memory_space=pltpu.VMEM), pl.BlockSpec((PAIR, count, depth), lambda step: (step, 0, 0))]
    return pl.pallas_call(
        lambda *refs: squares_kernel(full_width, *refs),
        grid=(chips // PAIR,),
        in_specs=specs,
        out_specs=pl.BlockSpec((count, 128), lambda step: (0, 0)),
        scratch_shapes=[pltpu.VMEM((count, 128), f32)],
        out_shape=jax.ShapeDtypeStruct((count, 128), f32),
        compiler_params=pltpu.CompilerParams(dimension_semantics=("arbitrary",), vmem_limit_bytes=28 << 20),
        cost_estimate=pl.CostEstimate(
            flops=4 * CORES * chips * count * depth, bytes_accessed=CORES * chips * count * depth * 2, transcendentals=0
        ),
        name="row_scaling",
    )(mine, other)


def first_kernel(chans, rows, ext_rows, total_rows, at, mine, other, scaling, w_all, mix, branch, ahead, joint, acc, turned):
    step = pl.program_id(0)
    lanes = 2 * chans
    count = mine.shape[1]
    core = at[0]
    total = 0
    for chip in range(PAIR):
        for part, place in ((mine[chip], core), (other[chip], 1 - core)):
            weight = w_all[CORES * chip + place]
            total = total + lax.dot_general(
                part, weight, (((1,), (1,)), ((), ())), preferred_element_type=f32
            )

    @pl.when(step == 0)
    def _():
        acc[...] = total

    @pl.when(step > 0)
    def _():
        acc[...] += total

    @pl.when(step == pl.num_programs(0) - 1)
    def _():
        code = at[1]
        both = (acc[:, :lanes] * scaling[...]).astype(bf16).astype(f32)
        running = both
        total = None
        for code_value, size in enumerate((1, 2, 4, 8)):
            running = running + pltpu.roll(running, count - size, 0)
            picked = pltpu.roll(running, size, 0)
            total = picked if total is None else jnp.where(code == code_value, picked, total)
        position = at[2] + lax.broadcasted_iota(jnp.int32, (count, lanes), 0)
        half = jnp.left_shift(1, code)
        counted = jnp.minimum(position + half, total_rows) - jnp.maximum(position - half, 0)
        counted = jnp.maximum(counted, 1).astype(f32)
        pooled = (total / counted - both).astype(bf16)
        mixed = jnp.dot(pooled, mix[...], preferred_element_type=f32)
        gated = mixed * (both / (1.0 + jnp.exp(-both)))
        turned[:count] = pltpu.roll(gated, count - REACH, 0)
        branch[...] = turned[...].T[:chans, :rows].astype(bf16)
        turned[:count] = pltpu.roll(acc[:, lanes:], count - REACH, 0)
        ahead[...] = turned[...].T[:, :rows]
        own = acc[ext_rows:, lanes:].astype(bf16)
        for i in range(joint.shape[0]):
            joint[i] = own


def first_layer(mine, other, scaling, gathered, mix, at, chans, ext_rows, total_rows, sp_size):
    chips, count, depth = mine.shape
    lanes = 2 * chans
    rows = ext_rows - 2 * REACH
    padded = -(-count // 128) * 128

    def block(step, at):
        return (step, 0, 0)

    def whole(step, at):
        return (0, 0)

    return pl.pallas_call(
        lambda *refs: first_kernel(chans, rows, ext_rows, total_rows, *refs),
        grid_spec=pltpu.PrefetchScalarGridSpec(
            num_scalar_prefetch=1,
            grid=(chips // PAIR,),
            in_specs=[
                pl.BlockSpec((PAIR, count, depth), block),
                pl.BlockSpec((PAIR, count, depth), block),
                pl.BlockSpec((count, lanes), whole),
                pl.BlockSpec((CORES * PAIR, 2 * lanes, depth), block),
                pl.BlockSpec((lanes, lanes), whole),
            ],
            out_specs=[
                pl.BlockSpec((chans, rows), whole),
                pl.BlockSpec((lanes, rows), whole),
                pl.BlockSpec((sp_size, count - ext_rows, lanes), lambda step, at: (0, 0, 0)),
            ],
            scratch_shapes=[
                pltpu.VMEM((count, 2 * lanes), f32),
                pltpu.VMEM((padded, lanes), f32),
            ],
        ),
        out_shape=[
            jax.ShapeDtypeStruct((chans, rows), bf16),
            jax.ShapeDtypeStruct((lanes, rows), f32),
            jax.ShapeDtypeStruct((sp_size, count - ext_rows, lanes), bf16),
        ],
        compiler_params=pltpu.CompilerParams(dimension_semantics=("arbitrary",), vmem_limit_bytes=50 << 20),
        cost_estimate=pl.CostEstimate(
            flops=CORES * chips * count * depth * 4 * lanes,
            bytes_accessed=CORES * chips * depth * 2 * (count + 2 * lanes),
            transcendentals=0,
        ),
        name="first_layer",
    )(at, mine, other, scaling, gathered, mix)


def mixed_branch(sums, scaling, mix, first_position, total_rows, code):
    rows = sums.shape[1] - 2 * REACH
    chans = sums.shape[0] // 2
    scaled = (sums * scaling[None, :]).astype(bf16).astype(f32)
    pool_in = scaled[chans:]
    gate = window(scaled[:chans], REACH, rows)
    position = first_position + jnp.arange(rows, dtype=jnp.int32)
    half = jnp.left_shift(1, code)
    counted = jnp.minimum(position + half, total_rows) - jnp.maximum(position - half, 0)
    counted = counted.astype(f32)
    running = pool_in
    total = None
    for code_value, size in enumerate((1, 2, 4, 8)):
        width = running.shape[1] - size
        running = window(running, 0, width) + window(running, size, width)
        picked = window(running, REACH - size, rows)
        total = picked if total is None else jnp.where(code == code_value, picked, total)
    pooled = (total / counted[None, :] - window(pool_in, REACH, rows)).astype(bf16)
    mixed = dot0(mix, pooled)
    return (mixed * jax.nn.silu(gate)).astype(bf16)


def local(hidden_in, norm_gain, w_pool_in, w_pool_gate, group_mix, w_out):
    rows, cols = hidden_in.shape
    chans = w_pool_in.shape[2]
    out_rows = w_out.shape[1]
    col_rank = lax.axis_index("tp")
    row_rank = lax.axis_index("sp")
    tp_size = lax.axis_size("tp")
    sp_size = lax.axis_size("sp")
    chips = tp_size // CORES
    core = jnp.bitwise_and(col_rank, CORES - 1)
    total_rows = rows * sp_size
    full_width = cols * tp_size
    code = jnp.bitwise_and(col_rank, 3)
    halo = 2 * REACH
    ext_rows = rows + 2 * halo
    lanes = 2 * chans

    packed = packed_weights(w_pool_gate.transpose(0, 2, 1), w_pool_in.transpose(0, 2, 1), w_out, norm_gain, row_rank)
    packed, hidden_in = lax.optimization_barrier((packed, hidden_in))
    gathered = lax.all_gather(packed, "sp", axis=0, tiled=False)

    def last_rows(gathered, layer):
        at = 2 * lanes + layer * out_rows
        return gathered[:, at : at + out_rows].reshape(chips, CORES * out_rows, cols)

    up = [(i, i + 1) for i in range(sp_size - 1)]
    down = [(j, i) for i, j in up]
    before = lax.ppermute(hidden_in[rows - halo :], "sp", up)
    after = lax.ppermute(hidden_in[:halo], "sp", down)
    block = jnp.concatenate([before, hidden_in, after, w_out[0]], axis=0)
    mine = same_core_blocks(block)
    other = swap_cores(mine)

    chip = col_rank // CORES
    ring = jnp.bitwise_and(chip + core, 1)

    def by_ring(array):
        size = array.shape[1] // CORES
        paired = array.reshape(chips // 2, 2 * CORES, size, array.shape[2])
        sides = []
        for c in (ring, 1 - ring):
            picked = [lax.dynamic_slice_in_dim(paired, at, 1, axis=1) for at in (c, CORES + 1 - c)]
            sides.append(jnp.concatenate(picked, axis=1).reshape(-1, array.shape[2]))
        return sides

    twins = [[CORES * i + (i + c) % CORES for i in range(chips)] for c in range(CORES)]

    def over_twins(branch):
        return lax.all_gather(branch, "tp", axis=0, tiled=True, axis_index_groups=twins)

    def product(weights, operands):
        return sum(dot0(weight, operand) for weight, operand in zip(weights, operands))

    mixes = [lax.dynamic_index_in_dim(group_mix[i], col_rank, 0, keepdims=False) for i in range(2)]

    mid_rows = rows + 2 * REACH
    start = row_rank * rows
    mix = jnp.pad(mixes[0], ((chans, 0), (0, chans)))
    scalars = jnp.stack([core, code, start - halo]).astype(jnp.int32)
    scaling = row_scaling(mine, other, full_width)
    branch, ahead, joint = first_layer(
        mine, other, scaling, gathered, mix, scalars, chans, ext_rows, total_rows, sp_size
    )
    joint = exchanged(joint, "sp")
    same = over_twins(branch)
    same, joint, gathered = lax.optimization_barrier((same, joint, gathered))
    joint = joint.reshape(chips, CORES * out_rows, lanes)
    other = swap_cores(same)
    pair = same, other
    delta = product(pair, by_ring(last_rows(gathered, 0)))
    resid = (block[REACH : REACH + mid_rows].astype(f32) + delta).astype(bf16)
    resid_f = resid.astype(f32)
    square_sum = sent_to_all(jnp.sum(resid_f * resid_f, axis=1), "tp").sum(axis=0)
    scaling = lax.rsqrt(square_sum / full_width + norm_eps)

    sums = ahead + product(by_ring(joint), pair)
    branch = mixed_branch(sums, scaling, mixes[1], start, total_rows, code)
    same = over_twins(branch)
    pair = same, swap_cores(same)
    resid = resid_f[REACH : REACH + rows] + product(pair, by_ring(last_rows(gathered, 1)))
    return resid.astype(bf16)


def solution(mesh):
    in_specs = (
        P(("grp", "sp"), "tp"),
        P(),
        P(None, "sp", "tp"),
        P(None, "sp", "tp"),
        P(),
        P(None, "sp", "tp"),
    )
    out_specs = P(("grp", "sp"), "tp")
    return jax.shard_map(local, mesh=mesh, in_specs=in_specs, out_specs=out_specs, check_vma=False)
```
